32 devices in a mesh: sp: 16 (over z, y, x), tp: 2 (over core).
Axes of the slice: x: 2, y: 2, z: 4, core: 2. Of those that a mesh axis runs over, the one named last changes fastest.
Arguments:
- tokens: bfloat16 [4096, 2048], P('sp'), may hold values from -6 to 6
- query_weight: bfloat16 [2, 2048, 512], P(None, None, 'tp'), may hold values from -0.125 to 0.125
- key_weight: bfloat16 [2, 2048, 512], P(None, None, 'tp'), may hold values from -0.125 to 0.125
- value_weight: bfloat16 [2, 2048, 512], P(None, None, 'tp'), may hold values from -0.125 to 0.125
- out_weight: bfloat16 [2, 512, 2048], replicated, may hold values from -1.5 to 1.5
- rel_table: float32 [2, 8, 257], P(None, 'tp'), may hold values from -5 to 262
- norm_gain: float32 [2, 2048], replicated, may hold values from 0.1 to 1.9
- norm_bias: float32 [2, 2048], replicated, may hold values from -1.5 to 1.5
Outputs:
- encoded: bfloat16 [4096, 2048], P('sp', 'tp')
The draws below stay inside these ranges and needn't reach their ends.
All inputs are finite; a program needn't handle non-finite values.
Results may differ from the reference program's by a relative error of at most 0.0095.
Values may be sent and summed in bfloat16 or wider, within the bound.
A program may use at most 64 MiB of HBM per device.

```python
import jax
import jax.numpy as jnp
from jax import lax

D = 2048
HEADS = 8
HEAD_DIM = 64
SEG = 64
LEFT = 4
CLIP = 128
LAYERS = 2
HW = 512
TOKENS = 4096


def draw_rel_table(key, part):
    shape = (LAYERS, HEADS, 2 * CLIP + 1)
    return jnp.clip(jax.random.normal(key, shape, jnp.float32), -5.0, 5.0)


def block_scale(key, dims, split, low, largest):
    level, own = 1.0, jax.random.fold_in(key, 6)
    for position, parts in split:
        draws = jnp.exp(jax.random.uniform(jax.random.fold_in(own, position), (parts,), jnp.float32, low / len(split), largest / len(split)))
        level = level * jnp.repeat(draws, dims[position] // parts).reshape([-1 if axis == position else 1 for axis in range(len(dims))])
    return level


def gaussian(key, shape, scale, most, cuts=(), held_as=jnp.bfloat16):
    level = block_scale(key, shape, cuts, -0.22, 0.18) if cuts else 1.0
    values = jax.random.normal(key, shape, jnp.float32) * scale * level
    return jnp.minimum(jnp.maximum(values, -most), most).astype(held_as)


def setup_inputs(seed: int = 0) -> dict:
    seeds = jax.random.split(jax.random.key(seed), 9)
    return {
        "tokens": gaussian(seeds[0], (TOKENS, D), 1.0, 6.0, ((0, 16),)),
        "query_weight": gaussian(seeds[1], (LAYERS, D, HW), D ** -0.5, 0.125, ((2, 2),)),
        "key_weight": gaussian(seeds[2], (LAYERS, D, HW), D ** -0.5, 0.125, ((2, 2),)),
        "value_weight": gaussian(seeds[3], (LAYERS, D, HW), D ** -0.5, 0.125, ((2, 2),)),
        "out_weight": gaussian(seeds[4], (LAYERS, HW, D), (HW // 32) ** -0.5, 1.5),
        "rel_table": draw_rel_table(jax.random.fold_in(seeds[8], 71), 0),
        "norm_gain": jnp.clip(1.0 + 0.18 * jax.random.normal(seeds[6], (LAYERS, D), jnp.float32), 0.1, 1.9),
        "norm_bias": gaussian(seeds[7], (LAYERS, D), 0.3, 1.5, (), jnp.float32),
    }


residual_scale = 2.0 ** 0.5
norm_eps = 1e-05
masked_score = -1e+30

def post_norm(previous, mixed, gain, shift):
    total = residual_scale * previous.astype(jnp.float32) + mixed
    mean = lax.optimization_barrier(jnp.mean(total, -1, keepdims=True))
    centred = total - mean
    variance = lax.optimization_barrier(jnp.mean(centred * centred, -1, keepdims=True))
    return (centred * lax.rsqrt(variance + norm_eps) * gain + shift).astype(jnp.bfloat16)

def band_attention(query, keys, values, table):
    reach = LEFT * SEG
    band = reach + SEG
    seg_count = TOKENS // SEG
    query3 = query.reshape(TOKENS, HEADS, HEAD_DIM)
    zeros = jnp.zeros((reach, HEADS, HEAD_DIM), jnp.bfloat16)
    padded_keys = jnp.concatenate([zeros, keys.reshape(TOKENS, HEADS, HEAD_DIM)], axis=0)
    padded_values = jnp.concatenate([zeros, values.reshape(TOKENS, HEADS, HEAD_DIM)], axis=0)
    distance = reach + jnp.arange(SEG, dtype=jnp.int32)[:, None] - jnp.arange(band, dtype=jnp.int32)[None, :]
    column = jnp.clip(distance, -CLIP, CLIP) + CLIP
    bias = table.astype(jnp.float32)[:, column]

    def one_segment(index):
        start = (index * SEG).astype(jnp.int32)
        query_block = lax.dynamic_slice_in_dim(query3, start, SEG, 0).astype(jnp.float32)
        key_band = lax.dynamic_slice_in_dim(padded_keys, start, band, 0).astype(jnp.float32)
        value_band = lax.dynamic_slice_in_dim(padded_values, start, band, 0).astype(jnp.float32)
        scores = jnp.einsum('qhd,khd->hqk', query_block, key_band) * HEAD_DIM ** (-0.5) + bias
        key_position = start - reach + jnp.arange(band, dtype=jnp.int32)
        scores = jnp.where((key_position >= 0)[None, None, :], scores, masked_score)
        peak = lax.optimization_barrier(jnp.max(scores, -1, keepdims=True))
        expo = jnp.exp(scores - peak)
        weights = (expo / lax.optimization_barrier(jnp.sum(expo, -1, keepdims=True))).astype(jnp.bfloat16)
        attended = jnp.einsum('hqk,khd->qhd', weights.astype(jnp.float32), value_band)
        return attended.astype(jnp.bfloat16)
    blocks = lax.map(one_segment, jnp.arange(seg_count, dtype=jnp.int32))
    return blocks.reshape(TOKENS, HEADS * HEAD_DIM)

def reference(tokens, query_weight, key_weight, value_weight, out_weight, rel_table, norm_gain, norm_bias):
    hidden = tokens
    for layer_index in range(LAYERS):
        query = jnp.dot(hidden, query_weight[layer_index], preferred_element_type=jnp.float32).astype(jnp.bfloat16)
        keys = jnp.dot(hidden, key_weight[layer_index], preferred_element_type=jnp.float32).astype(jnp.bfloat16)
        values = jnp.dot(hidden, value_weight[layer_index], preferred_element_type=jnp.float32).astype(jnp.bfloat16)
        attended = band_attention(query, keys, values, rel_table[layer_index])
        mixed = jnp.dot(attended, out_weight[layer_index], preferred_element_type=jnp.float32)
        hidden = post_norm(hidden, mixed, norm_gain[layer_index], norm_bias[layer_index])
    return hidden
```

```python
import functools

import jax
import jax.numpy as jnp
from jax import lax
from jax.experimental import pallas as pl
from jax.experimental.pallas import tpu as pltpu
from jax.sharding import PartitionSpec as P

SEG = 64
LEFT = 4
CLIP = 128
LAYERS = 2
LANES = 128

residual_scale = 2.0**0.5
norm_eps = 1e-05
masked_score = -1e30
MESH = pl.DeviceIdType.MESH


def kernel(
    sp_count,
    heads,
    tokens,
    wq_hbm,
    wk_hbm,
    wv_hbm,
    wo_hbm,
    table_hbm,
    gain_hbm,
    shift_hbm,
    out,
    x0,
    x1,
    wq,
    wk,
    wv,
    wo,
    table,
    gain,
    shift,
    query,
    kx,
    vx,
    att,
    total,
    bias,
    padded,
    x_sem,
    w_sem,
    small_sem,
    halo_send,
    halo_recv,
    pair_send,
    pair_recv,
):
    rows, model = x0.shape
    width = query.shape[2]
    head_size = width // heads
    reach = LEFT * SEG
    band = reach + SEG
    segments = rows // SEG
    sp = lax.axis_index("sp")
    tp = lax.axis_index("tp")
    has_next = sp < sp_count - 1
    has_prev = sp > 0

    def w_copy(kind, layer):
        source = (wk_hbm, wv_hbm, wq_hbm, wo_hbm)[kind]
        target = (wk, wv, wq, wo)[kind]
        return pltpu.make_async_copy(
            source.at[layer], target.at[layer], w_sem.at[kind, layer]
        )

    def x_copy(index, first, count):
        part = pl.ds(first, count)
        return pltpu.make_async_copy(tokens.at[part], x0.at[part], x_sem.at[index])

    x_last = x_copy(0, rows - SEG, SEG)
    x_rest = x_copy(1, 0, rows - SEG)
    small = [
        pltpu.make_async_copy(source, target, small_sem.at[index])
        for index, (source, target) in enumerate(
            ((table_hbm, table), (gain_hbm, gain), (shift_hbm, shift))
        )
    ]

    def halo_copy(kind, layer, seg):
        buffer = (kx, vx)[kind]
        return pltpu.make_async_remote_copy(
            src_ref=buffer.at[layer, pl.ds(reach + seg * SEG, SEG)],
            dst_ref=buffer.at[layer, pl.ds(seg * SEG, SEG)],
            send_sem=halo_send.at[kind, layer, seg],
            recv_sem=halo_recv.at[kind, layer, seg],
            device_id=(jnp.minimum(sp + 1, sp_count - 1), tp),
            device_id_type=MESH,
        )

    def pair_copy(layer, seg):
        block = att.at[layer, tp, pl.ds(seg * SEG, SEG)]
        return pltpu.make_async_remote_copy(
            src_ref=block,
            dst_ref=block,
            send_sem=pair_send.at[layer, seg],
            recv_sem=pair_recv.at[layer, seg],
            device_id=(sp, 1 - tp),
            device_id_type=MESH,
        )

    x_last.start()
    w_copy(0, 0).start()
    w_copy(1, 0).start()
    x_rest.start()
    w_copy(2, 0).start()

    barrier = pltpu.get_barrier_semaphore()
    pl.semaphore_signal(barrier, inc=1, device_id=(sp, 1 - tp), device_id_type=MESH)

    @pl.when(has_next)
    def _():
        pl.semaphore_signal(barrier, inc=1, device_id=(sp + 1, tp), device_id_type=MESH)

    @pl.when(has_prev)
    def _():
        pl.semaphore_signal(barrier, inc=1, device_id=(sp - 1, tp), device_id_type=MESH)

    @pl.when(jnp.logical_not(has_prev))
    def _():
        for layer in range(LAYERS):
            kx[layer, :reach, :] = jnp.zeros((reach, width), jnp.bfloat16)
            vx[layer, :reach, :] = jnp.zeros((reach, width), jnp.bfloat16)

    lane = lax.broadcasted_iota(jnp.int32, (1, width), 1)
    in_head = [
        (lane >= h * head_size) & (lane < (h + 1) * head_size) for h in range(heads)
    ]

    def build_bias():
        wide = bias.shape[2]
        size = padded.shape[1]
        padded[...] = jnp.zeros_like(padded)
        for layer in range(LAYERS):
            padded[layer * heads : (layer + 1) * heads, : table.shape[2]] = table[layer]
        place = lax.broadcasted_iota(jnp.int32, (size, wide), 1)
        source = lax.broadcasted_iota(jnp.int32, (size, wide), 0)
        onehot = (jnp.clip(band - 1 - place, -CLIP, CLIP) + CLIP == source).astype(jnp.float32)
        by_offset = jnp.dot(
            padded[...],
            onehot,
            precision=lax.Precision.HIGHEST,
            preferred_element_type=jnp.float32,
        )
        for layer in range(LAYERS):
            for h in range(heads):
                line = by_offset[layer * heads + h : layer * heads + h + 1, :]
                skewed = pltpu.roll(
                    jnp.broadcast_to(line, (SEG, wide)), wide - SEG + 1, 1, stride=1, stride_axis=0
                )
                bias[layer, h * SEG : (h + 1) * SEG, :] = skewed

    def rows_of(piece):
        return slice(piece[0] * SEG, piece[1] * SEG)

    def project(hidden, layer, part, kind):
        weight = (wk, wv, wq)[kind]
        return jnp.dot(
            hidden[part, :], weight[layer], preferred_element_type=jnp.float32
        ).astype(jnp.bfloat16)

    def keys_values(hidden, layer, piece):
        part = rows_of(piece)
        target = slice(reach + part.start, reach + part.stop)
        kx[layer, target, :] = project(hidden, layer, part, 0)
        vx[layer, target, :] = project(hidden, layer, part, 1)

        @pl.when(has_next)
        def _():
            for seg in range(*piece)[::-1]:
                halo_copy(0, layer, seg).start()
                halo_copy(1, layer, seg).start()

    def queries(hidden, layer, piece):
        first, last = piece[0] * SEG, piece[1] * SEG
        middle = (first + last) // 2
        for part in (slice(first, middle), slice(middle, last)):
            query[layer, part, :] = project(hidden, layer, part, 2) * jnp.bfloat16(
                head_size**-0.5
            )

    def wait_halo(layer, seg):
        @pl.when(has_prev)
        def _():
            halo_copy(0, layer, seg).wait_recv()
            halo_copy(1, layer, seg).wait_recv()

    def attend(layer, seg):
        column = lax.broadcasted_iota(jnp.int32, (1, band), 1)
        block = query[layer, seg * SEG : (seg + 1) * SEG, :]
        stacked = jnp.concatenate(
            [jnp.where(in_head[h], block, jnp.zeros_like(block)) for h in range(heads)], axis=0
        )
        key_band = kx[layer, seg * SEG : seg * SEG + band, :]
        value_band = vx[layer, seg * SEG : seg * SEG + band, :]
        scores = lax.dot_general(
            stacked, key_band, (((1,), (1,)), ((), ())), preferred_element_type=jnp.float32
        )
        outside = (column < reach - seg * SEG) & jnp.logical_not(has_prev)
        scores = jnp.where(outside, masked_score, scores + bias[layer, :, :band])
        peak = jnp.max(scores, -1, keepdims=True)
        expo = jnp.exp(scores - peak)
        norm = jnp.sum(expo, -1, keepdims=True)
        mixed = jnp.dot(
            expo.astype(jnp.bfloat16), value_band, preferred_element_type=jnp.float32
        )
        mixed = mixed * (1.0 / norm)
        own = mixed[:SEG, :]
        for h in range(1, heads):
            own = jnp.where(in_head[h], mixed[h * SEG : (h + 1) * SEG, :], own)
        att[layer, tp, seg * SEG : (seg + 1) * SEG, :] = own.astype(jnp.bfloat16)

    def half(layer, owner, seg):
        weight = wo[layer, pl.ds(pl.multiple_of(owner * width, width), width), :]
        return jnp.dot(
            att[layer, owner, seg * SEG : (seg + 1) * SEG, :],
            weight,
            preferred_element_type=jnp.float32,
        )

    def own_half(hidden, layer, seg):
        part = slice(seg * SEG, (seg + 1) * SEG)
        total[seg % 2] = half(layer, tp, seg) + residual_scale * hidden[part, :].astype(
            jnp.float32
        )

    def finish(layer, seg):
        total[seg % 2] += half(layer, 1 - tp, seg)
        step = 16
        for r in range(0, SEG, step):
            here = slice(seg * SEG + r, seg * SEG + r + step)
            value = total[seg % 2, r : r + step, :]
            mean = jnp.sum(value, -1, keepdims=True) * (1.0 / model)
            centred = value - mean
            variance = jnp.sum(centred * centred, -1, keepdims=True) * (1.0 / model)
            scale = lax.rsqrt(variance + norm_eps)
            if layer < LAYERS - 1:
                x1[here, :] = (
                    centred * scale * gain[layer : layer + 1, :] + shift[layer : layer + 1, :]
                ).astype(jnp.bfloat16)
            else:
                cols = pl.ds(pl.multiple_of(tp * (model // 2), model // 2), model // 2)
                out[here, :] = (
                    (total[seg % 2, r : r + step, cols] - mean)
                    * scale
                    * gain[layer : layer + 1, cols]
                    + shift[layer : layer + 1, cols]
                ).astype(jnp.bfloat16)

    last = segments - 1
    scope = jax.named_scope
    x_last.wait()
    w_copy(0, 0).wait()
    w_copy(1, 0).wait()
    with scope("barrier"):
        pl.semaphore_wait(barrier, 1 + has_next.astype(jnp.int32) + has_prev.astype(jnp.int32))
    with scope("kv_last"):
        keys_values(x0, 0, (last, segments))
    with scope("x_rest"):
        x_rest.wait()
    for copy in (w_copy(3, 0), *small):
        copy.start()
    with scope("kv_rest"):
        keys_values(x0, 0, (0, last))
    w_copy(2, 0).wait()
    with scope("queries"):
        queries(x0, 0, (0, segments))
    for kind in range(4):
        w_copy(kind, 1).start()
    for copy in small:
        copy.wait()
    with scope("bias"):
        build_bias()
    w_copy(3, 0).wait()

    hiddens = (x0, x1)
    for layer in range(LAYERS):
        waiting = None
        for seg in range(segments)[::-1]:
            with scope(f"halo_{layer}_{seg}"):
                wait_halo(layer, seg)
            with scope(f"attend_{layer}_{seg}"):
                attend(layer, seg)
                pair_copy(layer, seg).start()
                if waiting is not None:
                    own_half(hiddens[layer], layer, waiting)
            if waiting is not None:
                with scope(f"pair_{layer}_{waiting}"):
                    pair_copy(layer, waiting).wait_recv()
                with scope(f"finish_{layer}_{waiting}"):
                    finish(layer, waiting)
                if layer < LAYERS - 1:
                    if waiting == last:
                        w_copy(0, layer + 1).wait()
                        w_copy(1, layer + 1).wait()
                    with scope(f"kv_{layer}_{waiting}"):
                        keys_values(hiddens[layer + 1], layer + 1, (waiting, waiting + 1))
            waiting = seg
        with scope(f"own_{layer}"):
            own_half(hiddens[layer], layer, waiting)
        with scope(f"pair_{layer}_{waiting}"):
            pair_copy(layer, waiting).wait_recv()
        with scope(f"finish_{layer}_{waiting}"):
            finish(layer, waiting)
        if layer < LAYERS - 1:
            with scope(f"kv_{layer}_{waiting}"):
                keys_values(hiddens[layer + 1], layer + 1, (waiting, waiting + 1))
            w_copy(2, layer + 1).wait()
            w_copy(3, layer + 1).wait()
            with scope(f"queries_{layer}"):
                queries(hiddens[layer + 1], layer + 1, (0, segments))

    for layer in range(LAYERS):
        for seg in range(segments):
            pair_copy(layer, seg).wait_send()

    @pl.when(has_next)
    def _():
        for layer in range(LAYERS):
            for seg in range(segments):
                for kind in range(2):
                    halo_copy(kind, layer, seg).wait_send()


def body(
    sp_count, tokens, query_weight, key_weight, value_weight, out_weight, rel_table, norm_gain,
    norm_bias,
):
    rows, model = tokens.shape
    width = query_weight.shape[2]
    heads = rel_table.shape[1]
    reach = LEFT * SEG
    segments = rows // SEG
    wide = -(-(reach + 2 * SEG - 1) // LANES) * LANES
    size = -(-rel_table.shape[2] // LANES) * LANES
    hbm = pl.BlockSpec(memory_space=pltpu.MemorySpace.HBM)
    vmem = pl.BlockSpec(memory_space=pltpu.VMEM)
    bf16 = jnp.bfloat16
    return pl.pallas_call(
        functools.partial(kernel, sp_count, heads),
        out_shape=jax.ShapeDtypeStruct((rows, model // 2), bf16),
        in_specs=[hbm] * 8,
        out_specs=vmem,
        scratch_shapes=[
            pltpu.VMEM((rows, model), bf16),
            pltpu.VMEM((rows, model), bf16),
            pltpu.VMEM(query_weight.shape, bf16),
            pltpu.VMEM(key_weight.shape, bf16),
            pltpu.VMEM(value_weight.shape, bf16),
            pltpu.VMEM(out_weight.shape, bf16),
            pltpu.VMEM(rel_table.shape, jnp.float32),
            pltpu.VMEM(norm_gain.shape, jnp.float32),
            pltpu.VMEM(norm_bias.shape, jnp.float32),
            pltpu.VMEM((LAYERS, rows, width), bf16),
            pltpu.VMEM((LAYERS, reach + rows, width), bf16),
            pltpu.VMEM((LAYERS, reach + rows, width), bf16),
            pltpu.VMEM((LAYERS, 2, rows, width), bf16),
            pltpu.VMEM((2, SEG, model), jnp.float32),
            pltpu.VMEM((LAYERS, heads * SEG, wide), jnp.float32),
            pltpu.VMEM((-(-LAYERS * heads // 8) * 8, size), jnp.float32),
            pltpu.SemaphoreType.DMA((2,)),
            pltpu.SemaphoreType.DMA((4, LAYERS)),
            pltpu.SemaphoreType.DMA((3,)),
            pltpu.SemaphoreType.DMA((2, LAYERS, segments)),
            pltpu.SemaphoreType.DMA((2, LAYERS, segments)),
            pltpu.SemaphoreType.DMA((LAYERS, segments)),
            pltpu.SemaphoreType.DMA((LAYERS, segments)),
        ],
        compiler_params=pltpu.CompilerParams(
            collective_id=0, has_side_effects=True, vmem_limit_bytes=56000000
        ),
    )(
        *(
            pltpu.with_memory_space_constraint(operand, pltpu.MemorySpace.HBM)
            for operand in (
                tokens,
                query_weight,
                key_weight,
                value_weight,
                out_weight,
                rel_table,
                norm_gain,
                norm_bias,
            )
        )
    )


def solution(mesh):
    return jax.shard_map(
        functools.partial(body, mesh.shape["sp"]),
        mesh=mesh,
        in_specs=(
            P("sp", None),
            P(None, None, "tp"),
            P(None, None, "tp"),
            P(None, None, "tp"),
            P(),
            P(None, "tp", None),
            P(),
            P(),
        ),
        out_specs=P("sp", "tp"),
        check_vma=False,
    )
```

```python
import functools

import jax
import jax.numpy as jnp
from jax import lax
from jax.experimental import pallas as pl
from jax.experimental.pallas import tpu as pltpu
from jax.sharding import PartitionSpec as P

SEG = 64
LEFT = 4
CLIP = 128
LAYERS = 2
LANES = 128
CHUNKS = 4

residual_scale = 2.0**0.5
norm_eps = 1e-05
masked_score = -1e30
MESH = pl.DeviceIdType.MESH


def kernel(
    sp_count,
    heads,
    tokens,
    wq_hbm,
    wk_hbm,
    wv_hbm,
    wo_hbm,
    table_hbm,
    gain_hbm,
    shift_hbm,
    out,
    x0,
    x1,
    wq,
    wk,
    wv,
    wo,
    table,
    gain,
    shift,
    query,
    kx,
    vx,
    att,
    peer,
    total,
    bias,
    padded,
    x_sem,
    first_sem,
    w_sem,
    small_sem,
    halo_send,
    halo_recv,
    pair_send,
    pair_recv,
):
    rows, model = x0.shape
    width = query.shape[2]
    head_size = width // heads
    reach = LEFT * SEG
    band = reach + SEG
    segments = rows // SEG
    sp = lax.axis_index("sp")
    tp = lax.axis_index("tp")
    has_next = sp < sp_count - 1
    has_prev = sp > 0

    def first_copy(kind, index):
        size = model // CHUNKS
        part = pl.ds(index * size, size)
        return pltpu.make_async_copy(
            (wk_hbm, wv_hbm)[kind].at[0, part],
            (wk, wv)[kind].at[0, part],
            first_sem.at[kind, index],
        )

    def w_copy(kind, layer):
        if kind < 3:
            source = (wk_hbm, wv_hbm, wq_hbm)[kind].at[layer]
            target = (wk, wv, wq)[kind].at[layer]
        else:
            owner = (tp, 1 - tp)[kind - 3]
            part = pl.ds(pl.multiple_of(owner * width, width), width)
            source = wo_hbm.at[layer, part]
            target = wo.at[layer, kind - 3]
        return pltpu.make_async_copy(source, target, w_sem.at[kind, layer])

    def x_copy(index, first, count):
        part = pl.ds(first, count)
        return pltpu.make_async_copy(tokens.at[part], x0.at[part], x_sem.at[index])

    x_last = x_copy(0, rows - SEG, SEG)
    x_rest = x_copy(1, 0, rows - SEG)
    small = [
        pltpu.make_async_copy(source, target, small_sem.at[index])
        for index, (source, target) in enumerate(
            ((table_hbm, table), (gain_hbm, gain), (shift_hbm, shift))
        )
    ]

    def halo_copy(kind, layer, seg):
        buffer = (kx, vx)[kind]
        return pltpu.make_async_remote_copy(
            src_ref=buffer.at[layer, pl.ds(reach + seg * SEG, SEG)],
            dst_ref=buffer.at[layer, pl.ds(seg * SEG, SEG)],
            send_sem=halo_send.at[kind, layer, seg],
            recv_sem=halo_recv.at[kind, layer, seg],
            device_id=(jnp.minimum(sp + 1, sp_count - 1), tp),
            device_id_type=MESH,
        )

    def pair_copy(layer, seg):
        part = pl.ds(seg * SEG, SEG)
        return pltpu.make_async_remote_copy(
            src_ref=att.at[layer, part],
            dst_ref=peer.at[layer, part],
            send_sem=pair_send.at[layer, seg],
            recv_sem=pair_recv.at[layer, seg],
            device_id=(sp, 1 - tp),
            device_id_type=MESH,
        )

    x_last.start()
    first = [first_copy(kind, index) for kind in range(2) for index in range(CHUNKS)]
    for copy in first:
        copy.start()
    x_rest.start()
    w_copy(2, 0).start()

    barrier = pltpu.get_barrier_semaphore()
    pl.semaphore_signal(barrier, inc=1, device_id=(sp, 1 - tp), device_id_type=MESH)

    @pl.when(has_prev)
    def _():
        pl.semaphore_signal(barrier, inc=1, device_id=(sp - 1, tp), device_id_type=MESH)

    @pl.when(jnp.logical_not(has_prev))
    def _():
        for layer in range(LAYERS):
            kx[layer, :reach, :] = jnp.zeros((reach, width), jnp.bfloat16)
            vx[layer, :reach, :] = jnp.zeros((reach, width), jnp.bfloat16)

    def build_bias():
        wide = bias.shape[2]
        size = padded.shape[1]
        padded[...] = jnp.zeros_like(padded)
        for layer in range(LAYERS):
            padded[layer * heads : (layer + 1) * heads, : table.shape[2]] = table[layer]
        place = lax.broadcasted_iota(jnp.int32, (size, wide), 1)
        source = lax.broadcasted_iota(jnp.int32, (size, wide), 0)
        onehot = (jnp.clip(band - 1 - place, -CLIP, CLIP) + CLIP == source).astype(jnp.float32)
        by_offset = jnp.dot(
            padded[...],
            onehot,
            precision=lax.Precision.HIGHEST,
            preferred_element_type=jnp.float32,
        )
        for layer in range(LAYERS):
            for h in range(heads):
                line = by_offset[layer * heads + h : layer * heads + h + 1, :]
                skewed = pltpu.roll(
                    jnp.broadcast_to(line, (SEG, wide)), wide - SEG + 1, 1, stride=1, stride_axis=0
                )
                bias[layer, h * SEG : (h + 1) * SEG, :] = skewed

    def rows_of(piece):
        return slice(piece[0] * SEG, piece[1] * SEG)

    def project(hidden, layer, part, kind):
        weight = (wk, wv, wq)[kind]
        return jnp.dot(
            hidden[part, :], weight[layer], preferred_element_type=jnp.float32
        ).astype(jnp.bfloat16)

    def keys_values(hidden, layer, piece):
        part = rows_of(piece)
        target = slice(reach + part.start, reach + part.stop)
        kx[layer, target, :] = project(hidden, layer, part, 0)
        vx[layer, target, :] = project(hidden, layer, part, 1)

        @pl.when(has_next)
        def _():
            for seg in range(*piece)[::-1]:
                halo_copy(0, layer, seg).start()
                halo_copy(1, layer, seg).start()

    def project_split(hidden, layer, part, kind):
        weight = (wk, wv, wq)[kind]
        return [
            jnp.dot(
                hidden[part, :],
                weight[layer, :, first : first + LANES],
                preferred_element_type=jnp.float32,
            ).astype(jnp.bfloat16)
            for first in range(0, width, LANES)
        ]

    def keys(hidden, layer, seg):
        target = slice(reach + seg * SEG, reach + (seg + 1) * SEG)
        for group, block in enumerate(
            project_split(hidden, layer, slice(seg * SEG, (seg + 1) * SEG), 0)
        ):
            kx[layer, target, group * LANES : (group + 1) * LANES] = block

        @pl.when(has_next)
        def _():
            halo_copy(0, layer, seg).start()

    def values(hidden, layer, seg):
        target = slice(reach + seg * SEG, reach + (seg + 1) * SEG)
        for group, block in enumerate(
            project_split(hidden, layer, slice(seg * SEG, (seg + 1) * SEG), 1)
        ):
            vx[layer, target, group * LANES : (group + 1) * LANES] = block

        @pl.when(has_next)
        def _():
            halo_copy(1, layer, seg).start()

    def queries(hidden, layer, piece):
        first, last = piece[0] * SEG, piece[1] * SEG
        middle = (first + last) // 2 if last - first > SEG else last
        for part in (slice(first, middle), slice(middle, last)):
            if part.start == part.stop:
                continue
            query[layer, part, :] = project(hidden, layer, part, 2) * jnp.bfloat16(
                head_size**-0.5
            )

    def wait_halo(layer, seg, kind=None):
        @pl.when(has_prev)
        def _():
            for each in (0, 1) if kind is None else (kind,):
                halo_copy(each, layer, seg).wait_recv()

    pair = LANES // head_size
    lane = lax.broadcasted_iota(jnp.int32, (1, LANES), 1)
    in_pair = [
        (lane >= h * head_size) & (lane < (h + 1) * head_size) for h in range(pair)
    ]

    def scores(layer, seg):
        column = lax.broadcasted_iota(jnp.int32, (1, band), 1)
        outside = (column < reach - seg * SEG) & jnp.logical_not(has_prev)
        results = []
        for group in range(width // LANES):
            lanes = slice(group * LANES, (group + 1) * LANES)
            block = query[layer, seg * SEG : (seg + 1) * SEG, lanes]
            stacked = jnp.concatenate(
                [jnp.where(in_pair[h], block, jnp.zeros_like(block)) for h in range(pair)], axis=0
            )
            raw = lax.dot_general(
                stacked,
                kx[layer, seg * SEG : seg * SEG + band, lanes],
                (((1,), (1,)), ((), ())),
                preferred_element_type=jnp.float32,
            )
            lines = slice(group * pair * SEG, (group + 1) * pair * SEG)
            results.append(jnp.where(outside, masked_score, raw + bias[layer, lines, :band]))
        return results

    def weigh(layer, seg, results):
        for group, raw in enumerate(results):
            lanes = slice(group * LANES, (group + 1) * LANES)
            peak = jnp.max(raw, -1, keepdims=True)
            expo = jnp.exp(raw - peak)
            norm = jnp.sum(expo, -1, keepdims=True)
            mixed = jnp.dot(
                expo.astype(jnp.bfloat16),
                vx[layer, seg * SEG : seg * SEG + band, lanes],
                preferred_element_type=jnp.float32,
            )
            mixed = mixed * (1.0 / norm)
            own = mixed[:SEG, :]
            for h in range(1, pair):
                own = jnp.where(in_pair[h], mixed[h * SEG : (h + 1) * SEG, :], own)
            att[layer, seg * SEG : (seg + 1) * SEG, lanes] = own.astype(jnp.bfloat16)

    def half(layer, seg, source, index):
        return jnp.dot(
            source[layer, seg * SEG : (seg + 1) * SEG, :],
            wo[layer, index],
            preferred_element_type=jnp.float32,
        )

    def own_half(hidden, layer, seg):
        part = slice(seg * SEG, (seg + 1) * SEG)
        total[seg % 2] = half(layer, seg, att, 0) + residual_scale * hidden[part, :].astype(
            jnp.float32
        )

    def other_half(layer, seg):
        total[seg % 2] += half(layer, seg, peer, 1)

    def finish(layer, seg):
        step = 16
        for r in range(0, SEG, step):
            here = slice(seg * SEG + r, seg * SEG + r + step)
            value = total[seg % 2, r : r + step, :]
            mean = jnp.sum(value, -1, keepdims=True) * (1.0 / model)
            centred = value - mean
            variance = jnp.sum(centred * centred, -1, keepdims=True) * (1.0 / model)
            scale = lax.rsqrt(variance + norm_eps)
            if layer < LAYERS - 1:
                x1[here, :] = (
                    centred * scale * gain[layer : layer + 1, :] + shift[layer : layer + 1, :]
                ).astype(jnp.bfloat16)
            else:
                cols = pl.ds(pl.multiple_of(tp * (model // 2), model // 2), model // 2)
                out[here, :] = (
                    (total[seg % 2, r : r + step, cols] - mean)
                    * scale
                    * gain[layer : layer + 1, cols]
                    + shift[layer : layer + 1, cols]
                ).astype(jnp.bfloat16)

    last = segments - 1
    scope = jax.named_scope
    with scope("x_last"):
        x_last.wait()
    with scope("w_k"):
        for copy in first[:CHUNKS]:
            copy.wait()
    with scope("barrier"):
        pl.semaphore_wait(barrier, 1 + has_next.astype(jnp.int32))
    with scope("k_last"):
        keys(x0, 0, last)
    with scope("w_v"):
        for copy in first[CHUNKS:]:
            copy.wait()
    with scope("v_last"):
        values(x0, 0, last)
    with scope("x_rest"):
        x_rest.wait()
    for copy in (*small, w_copy(3, 0), w_copy(4, 0)):
        copy.start()
    with scope("kv_rest"):
        keys_values(x0, 0, (0, last))
    w_copy(2, 0).wait()
    with scope("queries"):
        queries(x0, 0, (0, segments))
    for kind in range(5):
        w_copy(kind, 1).start()
    for copy in small:
        copy.wait()
    with scope("bias"):
        build_bias()
    w_copy(3, 0).wait()
    w_copy(4, 0).wait()

    hiddens = (x0, x1)
    for layer in range(LAYERS):
        hidden = hiddens[layer]
        more = layer < LAYERS - 1
        with scope(f"halo_{layer}_{last}"):
            wait_halo(layer, last)
        with scope(f"attend_{layer}_{last}"):
            weigh(layer, last, scores(layer, last))
        pair_copy(layer, last).start()
        if more:
            with scope(f"own_{layer}_{last}"):
                own_half(hidden, layer, last)
            for kind in range(5):
                w_copy(kind, layer + 1).wait()
            for seg in range(segments)[::-1]:
                if seg > 0:
                    with scope(f"halo_{layer}_{seg - 1}"):
                        wait_halo(layer, seg - 1)
                with scope(f"pair_{layer}_{seg}"):
                    pair_copy(layer, seg).wait_recv()
                with scope(f"block_{layer}_{seg}"):
                    if seg > 0:
                        results = scores(layer, seg - 1)
                    other_half(layer, seg)
                    if seg > 0:
                        weigh(layer, seg - 1, results)
                    finish(layer, seg)
                if seg > 0:
                    pair_copy(layer, seg - 1).start()
                with scope(f"kv_{layer}_{seg}"):
                    keys_values(hiddens[layer + 1], layer + 1, (seg, seg + 1))
                with scope(f"own_{layer}_{seg}"):
                    if seg > 0:
                        own_half(hidden, layer, seg - 1)
                    else:
                        queries(hiddens[layer + 1], layer + 1, (0, segments))
        else:
            done = last
            for seg in range(last)[::-1]:
                with scope(f"halo_{layer}_{seg}"):
                    wait_halo(layer, seg, 0)
                    if seg > 0:
                        wait_halo(layer, seg, 1)
                if 0 < seg < last - 1:
                    with scope(f"pair_{layer}_{done}"):
                        pair_copy(layer, done).wait_recv()
                with scope(f"block_{layer}_{seg}"):
                    results = scores(layer, seg)
                    if seg == last - 1:
                        own_half(hidden, layer, last)
                    elif seg > 0:
                        other_half(layer, done)
                    else:
                        own_half(hidden, layer, seg + 1)
                    if seg == 0:
                        with scope("halo_v"):
                            wait_halo(layer, seg, 1)
                    weigh(layer, seg, results)
                    if 0 < seg < last - 1:
                        finish(layer, done)
                pair_copy(layer, seg).start()
                if 0 < seg < last - 1:
                    done = done - 1
                    with scope(f"own_{layer}_{done}"):
                        own_half(hidden, layer, done)
                    if seg == 1:
                        with scope(f"pair_{layer}_{done}"):
                            pair_copy(layer, done).wait_recv()
                        with scope(f"finish_{layer}_{done}"):
                            other_half(layer, done)
                            finish(layer, done)
                        done = done - 1
            while done >= 0:
                if done == 0:
                    with scope(f"own_{layer}_{done}"):
                        own_half(hidden, layer, done)
                with scope(f"pair_{layer}_{done}"):
                    pair_copy(layer, done).wait_recv()
                with scope(f"finish_{layer}_{done}"):
                    other_half(layer, done)
                    finish(layer, done)
                done = done - 1

    for layer in range(LAYERS):
        for seg in range(segments):
            pair_copy(layer, seg).wait_send()

    @pl.when(has_next)
    def _():
        for layer in range(LAYERS):
            for seg in range(segments):
                for kind in range(2):
                    halo_copy(kind, layer, seg).wait_send()


def body(
    sp_count, tokens, query_weight, key_weight, value_weight, out_weight, rel_table, norm_gain,
    norm_bias,
):
    rows, model = tokens.shape
    width = query_weight.shape[2]
    heads = rel_table.shape[1]
    reach = LEFT * SEG
    segments = rows // SEG
    wide = -(-(reach + 2 * SEG - 1) // LANES) * LANES
    size = -(-rel_table.shape[2] // LANES) * LANES
    hbm = pl.BlockSpec(memory_space=pltpu.MemorySpace.HBM)
    vmem = pl.BlockSpec(memory_space=pltpu.VMEM)
    bf16 = jnp.bfloat16
    return pl.pallas_call(
        functools.partial(kernel, sp_count, heads),
        out_shape=jax.ShapeDtypeStruct((rows, model // 2), bf16),
        in_specs=[hbm] * 8,
        out_specs=vmem,
        scratch_shapes=[
            pltpu.VMEM((rows, model), bf16),
            pltpu.VMEM((rows, model), bf16),
            pltpu.VMEM(query_weight.shape, bf16),
            pltpu.VMEM(key_weight.shape, bf16),
            pltpu.VMEM(value_weight.shape, bf16),
            pltpu.VMEM((LAYERS, 2, width, model), bf16),
            pltpu.VMEM(rel_table.shape, jnp.float32),
            pltpu.VMEM(norm_gain.shape, jnp.float32),
            pltpu.VMEM(norm_bias.shape, jnp.float32),
            pltpu.VMEM((LAYERS, rows, width), bf16),
            pltpu.VMEM((LAYERS, reach + rows, width), bf16),
            pltpu.VMEM((LAYERS, reach + rows, width), bf16),
            pltpu.VMEM((LAYERS, rows, width), bf16),
            pltpu.VMEM((LAYERS, rows, width), bf16),
            pltpu.VMEM((2, SEG, model), jnp.float32),
            pltpu.VMEM((LAYERS, heads * SEG, wide), jnp.float32),
            pltpu.VMEM((-(-LAYERS * heads // 8) * 8, size), jnp.float32),
            pltpu.SemaphoreType.DMA((2,)),
            pltpu.SemaphoreType.DMA((2, CHUNKS)),
            pltpu.SemaphoreType.DMA((5, LAYERS)),
            pltpu.SemaphoreType.DMA((3,)),
            pltpu.SemaphoreType.DMA((2, LAYERS, segments)),
            pltpu.SemaphoreType.DMA((2, LAYERS, segments)),
            pltpu.SemaphoreType.DMA((LAYERS, segments)),
            pltpu.SemaphoreType.DMA((LAYERS, segments)),
        ],
        compiler_params=pltpu.CompilerParams(
            collective_id=0, has_side_effects=True, vmem_limit_bytes=56000000
        ),
    )(
        *(
            pltpu.with_memory_space_constraint(operand, pltpu.MemorySpace.HBM)
            for operand in (
                tokens,
                query_weight,
                key_weight,
                value_weight,
                out_weight,
                rel_table,
                norm_gain,
                norm_bias,
            )
        )
    )


def solution(mesh):
    return jax.shard_map(
        functools.partial(body, mesh.shape["sp"]),
        mesh=mesh,
        in_specs=(
            P("sp", None),
            P(None, None, "tp"),
            P(None, None, "tp"),
            P(None, None, "tp"),
            P(),
            P(None, "tp", None),
            P(),
            P(),
        ),
        out_specs=P("sp", "tp"),
        check_vma=False,
    )
```

```python
import functools

import jax
import jax.numpy as jnp
from jax import lax
from jax.experimental import pallas as pl
from jax.experimental.pallas import tpu as pltpu
from jax.sharding import PartitionSpec as P

SEG = 64
LEFT = 4
CLIP = 128
LAYERS = 2
LANES = 128
CHUNKS = 4

residual_scale = 2.0**0.5
norm_eps = 1e-05
masked_score = -1e30
MESH = pl.DeviceIdType.MESH


def kernel(
    sp_count,
    heads,
    tokens,
    wq_hbm,
    wk_hbm,
    wv_hbm,
    wo_hbm,
    table_hbm,
    gain_hbm,
    shift_hbm,
    out,
    x0,
    x1,
    wq,
    wk,
    wv,
    wo,
    table,
    gain,
    shift,
    query,
    kx,
    vx,
    att,
    peer,
    total,
    bias,
    padded,
    x_sem,
    first_sem,
    w_sem,
    small_sem,
    halo_send,
    halo_recv,
    pair_send,
    pair_recv,
):
    rows, model = x0.shape
    width = query.shape[2]
    head_size = width // heads
    reach = LEFT * SEG
    band = reach + SEG
    segments = rows // SEG
    sp = lax.axis_index("sp")
    tp = lax.axis_index("tp")
    has_next = sp < sp_count - 1
    has_prev = sp > 0

    def first_copy(kind, index):
        size = model // CHUNKS
        part = pl.ds(index * size, size)
        return pltpu.make_async_copy(
            (wk_hbm, wv_hbm)[kind].at[0, part],
            (wk, wv)[kind].at[0, part],
            first_sem.at[kind, index],
        )

    def w_copy(kind, layer):
        if kind < 3:
            source = (wk_hbm, wv_hbm, wq_hbm)[kind].at[layer]
            target = (wk, wv, wq)[kind].at[layer]
        else:
            owner = (tp, 1 - tp)[kind - 3]
            part = pl.ds(pl.multiple_of(owner * width, width), width)
            source = wo_hbm.at[layer, part]
            target = wo.at[layer, kind - 3]
        return pltpu.make_async_copy(source, target, w_sem.at[kind, layer])

    def x_copy(index, first, count):
        part = pl.ds(first, count)
        return pltpu.make_async_copy(tokens.at[part], x0.at[part], x_sem.at[index])

    x_last = x_copy(0, rows - SEG, SEG)
    x_rest = x_copy(1, 0, rows - SEG)
    small = [
        pltpu.make_async_copy(source, target, small_sem.at[index])
        for index, (source, target) in enumerate(
            ((table_hbm, table), (gain_hbm, gain), (shift_hbm, shift))
        )
    ]

    def halo_copy(kind, layer, seg):
        buffer = (kx, vx)[kind]
        return pltpu.make_async_remote_copy(
            src_ref=buffer.at[layer, pl.ds(reach + seg * SEG, SEG)],
            dst_ref=buffer.at[layer, pl.ds(seg * SEG, SEG)],
            send_sem=halo_send.at[kind, layer, seg],
            recv_sem=halo_recv.at[kind, layer, seg],
            device_id=(jnp.minimum(sp + 1, sp_count - 1), tp),
            device_id_type=MESH,
        )

    def pair_copy(layer, seg):
        part = pl.ds(seg * SEG, SEG)
        return pltpu.make_async_remote_copy(
            src_ref=att.at[layer, part],
            dst_ref=peer.at[layer, part],
            send_sem=pair_send.at[layer, seg],
            recv_sem=pair_recv.at[layer, seg],
            device_id=(sp, 1 - tp),
            device_id_type=MESH,
        )

    barrier = pltpu.get_barrier_semaphore()
    pl.semaphore_signal(barrier, inc=1, device_id=(sp, 1 - tp), device_id_type=MESH)

    @pl.when(has_prev)
    def _():
        pl.semaphore_signal(barrier, inc=1, device_id=(sp - 1, tp), device_id_type=MESH)

    x_last.start()
    first = [first_copy(kind, index) for kind in range(2) for index in range(CHUNKS)]
    for copy in first[:CHUNKS]:
        copy.start()
    pl.delay(200)
    for copy in first[CHUNKS:]:
        copy.start()
    x_rest.start()
    w_copy(2, 0).start()

    @pl.when(jnp.logical_not(has_prev))
    def _():
        for layer in range(LAYERS):
            kx[layer, :reach, :] = jnp.zeros((reach, width), jnp.bfloat16)
            vx[layer, :reach, :] = jnp.zeros((reach, width), jnp.bfloat16)

    def build_bias():
        wide = bias.shape[2]
        size = padded.shape[1]
        padded[...] = jnp.zeros_like(padded)
        for layer in range(LAYERS):
            padded[layer * heads : (layer + 1) * heads, : table.shape[2]] = table[layer]
        place = lax.broadcasted_iota(jnp.int32, (size, wide), 1)
        source = lax.broadcasted_iota(jnp.int32, (size, wide), 0)
        onehot = (jnp.clip(band - 1 - place, -CLIP, CLIP) + CLIP == source).astype(jnp.float32)
        by_offset = jnp.dot(
            padded[...],
            onehot,
            precision=lax.Precision.HIGHEST,
            preferred_element_type=jnp.float32,
        )
        for layer in range(LAYERS):
            for h in range(heads):
                line = by_offset[layer * heads + h : layer * heads + h + 1, :]
                skewed = pltpu.roll(
                    jnp.broadcast_to(line, (SEG, wide)), wide - SEG + 1, 1, stride=1, stride_axis=0
                )
                bias[layer, h * SEG : (h + 1) * SEG, :] = skewed

    def rows_of(piece):
        return slice(piece[0] * SEG, piece[1] * SEG)

    def project(hidden, layer, part, kind):
        weight = (wk, wv, wq)[kind]
        return jnp.dot(
            hidden[part, :], weight[layer], preferred_element_type=jnp.float32
        ).astype(jnp.bfloat16)

    def keys_values(hidden, layer, piece):
        part = rows_of(piece)
        target = slice(reach + part.start, reach + part.stop)
        kx[layer, target, :] = project(hidden, layer, part, 0)
        vx[layer, target, :] = project(hidden, layer, part, 1)

        @pl.when(has_next)
        def _():
            for seg in range(*piece)[::-1]:
                halo_copy(0, layer, seg).start()
                halo_copy(1, layer, seg).start()

    def project_split(hidden, layer, part, kind):
        weight = (wk, wv, wq)[kind]
        return [
            jnp.dot(
                hidden[part, :],
                weight[layer, :, first : first + LANES],
                preferred_element_type=jnp.float32,
            ).astype(jnp.bfloat16)
            for first in range(0, width, LANES)
        ]

    def store_keys(hidden, layer, seg):
        target = slice(reach + seg * SEG, reach + (seg + 1) * SEG)
        for group, block in enumerate(
            project_split(hidden, layer, slice(seg * SEG, (seg + 1) * SEG), 0)
        ):
            kx[layer, target, group * LANES : (group + 1) * LANES] = block

    def values(hidden, layer, seg):
        target = slice(reach + seg * SEG, reach + (seg + 1) * SEG)
        for group, block in enumerate(
            project_split(hidden, layer, slice(seg * SEG, (seg + 1) * SEG), 1)
        ):
            vx[layer, target, group * LANES : (group + 1) * LANES] = block

        @pl.when(has_next)
        def _():
            halo_copy(1, layer, seg).start()

    def queries_split(hidden, layer, seg):
        part = slice(seg * SEG, (seg + 1) * SEG)
        for group, block in enumerate(project_split(hidden, layer, part, 2)):
            query[layer, part, group * LANES : (group + 1) * LANES] = block * jnp.bfloat16(
                head_size**-0.5
            )

    def queries(hidden, layer, piece):
        first, last = piece[0] * SEG, piece[1] * SEG
        middle = (first + last) // 2 if last - first > SEG else last
        for part in (slice(first, middle), slice(middle, last)):
            if part.start == part.stop:
                continue
            query[layer, part, :] = project(hidden, layer, part, 2) * jnp.bfloat16(
                head_size**-0.5
            )

    def wait_halo(layer, seg, kind=None):
        @pl.when(has_prev)
        def _():
            for each in (0, 1) if kind is None else (kind,):
                halo_copy(each, layer, seg).wait_recv()

    pair = LANES // head_size
    lane = lax.broadcasted_iota(jnp.int32, (1, LANES), 1)
    in_pair = [
        (lane >= h * head_size) & (lane < (h + 1) * head_size) for h in range(pair)
    ]

    def scores(layer, seg):
        column = lax.broadcasted_iota(jnp.int32, (1, band), 1)
        outside = (column < reach - seg * SEG) & jnp.logical_not(has_prev)
        results = []
        for group in range(width // LANES):
            lanes = slice(group * LANES, (group + 1) * LANES)
            block = query[layer, seg * SEG : (seg + 1) * SEG, lanes]
            stacked = jnp.concatenate(
                [jnp.where(in_pair[h], block, jnp.zeros_like(block)) for h in range(pair)], axis=0
            )
            raw = lax.dot_general(
                stacked,
                kx[layer, seg * SEG : seg * SEG + band, lanes],
                (((1,), (1,)), ((), ())),
                preferred_element_type=jnp.float32,
            )
            lines = slice(group * pair * SEG, (group + 1) * pair * SEG)
            results.append(jnp.where(outside, masked_score, raw + bias[layer, lines, :band]))
        return results

    def soften(results):
        softened = []
        for raw in results:
            expo = jnp.exp(raw - jnp.max(raw, -1, keepdims=True))
            norm = jnp.sum(expo, -1, keepdims=True)
            softened.append((expo.astype(jnp.bfloat16), 1.0 / norm))
        return softened

    def weigh(layer, seg, softened):
        for group, (expo, inverse) in enumerate(softened):
            lanes = slice(group * LANES, (group + 1) * LANES)
            mixed = jnp.dot(
                expo,
                vx[layer, seg * SEG : seg * SEG + band, lanes],
                preferred_element_type=jnp.float32,
            )
            mixed = mixed * inverse
            own = mixed[:SEG, :]
            for h in range(1, pair):
                own = jnp.where(in_pair[h], mixed[h * SEG : (h + 1) * SEG, :], own)
            att[layer, seg * SEG : (seg + 1) * SEG, lanes] = own.astype(jnp.bfloat16)

    def half(layer, piece, source, index):
        return jnp.dot(
            source[layer, rows_of(piece), :],
            wo[layer, index],
            preferred_element_type=jnp.float32,
        )

    def own_half(hidden, layer, piece):
        part = rows_of(piece)
        total[part, :] = half(layer, piece, att, 0) + residual_scale * hidden[part, :].astype(
            jnp.float32
        )

    def other_half(layer, piece):
        total[rows_of(piece), :] += half(layer, piece, peer, 1)

    def finish(layer, piece):
        step = 16
        part = rows_of(piece)
        for r in range(part.start, part.stop, step):
            here = slice(r, r + step)
            value = total[here, :]
            mean = jnp.sum(value, -1, keepdims=True) * (1.0 / model)
            centred = value - mean
            variance = jnp.sum(centred * centred, -1, keepdims=True) * (1.0 / model)
            scale = lax.rsqrt(variance + norm_eps)
            if layer < LAYERS - 1:
                x1[here, :] = (
                    centred * scale * gain[layer : layer + 1, :] + shift[layer : layer + 1, :]
                ).astype(jnp.bfloat16)
            else:
                cols = pl.ds(pl.multiple_of(tp * (model // 2), model // 2), model // 2)
                out[here, :] = (
                    (total[here, cols] - mean) * scale * gain[layer : layer + 1, cols]
                    + shift[layer : layer + 1, cols]
                ).astype(jnp.bfloat16)

    last = segments - 1
    scope = jax.named_scope
    with scope("x_last"):
        x_last.wait()
    with scope("w_k"):
        for copy in first[:CHUNKS]:
            copy.wait()
    with scope("k_last"):
        store_keys(x0, 0, last)
    with scope("barrier"):
        pl.semaphore_wait(barrier, 1 + has_next.astype(jnp.int32))

    @pl.when(has_next)
    def _():
        halo_copy(0, 0, last).start()

    with scope("w_v"):
        for copy in first[CHUNKS:]:
            copy.wait()
    with scope("v_last"):
        values(x0, 0, last)
    with scope("x_rest"):
        x_rest.wait()
    for copy in (*small, w_copy(3, 0), w_copy(4, 0)):
        copy.start()
    with scope("kv_rest"):
        keys_values(x0, 0, (0, last))
    w_copy(2, 0).wait()
    with scope("queries"):
        queries(x0, 0, (0, segments))
    for kind in range(5):
        w_copy(kind, 1).start()
    for copy in small:
        copy.wait()
    with scope("bias"):
        build_bias()
    w_copy(3, 0).wait()
    w_copy(4, 0).wait()

    def one(seg):
        return (seg, seg + 1)

    hiddens = (x0, x1)
    for layer in range(LAYERS - 1):
        hidden, following = hiddens[layer], hiddens[layer + 1]
        with scope(f"k_{layer}_{last}"):
            wait_halo(layer, last, 0)
        with scope(f"soften_{layer}_{last}"):
            softened = soften(scores(layer, last))
        with scope(f"v_{layer}_{last}"):
            wait_halo(layer, last, 1)
        with scope(f"weigh_{layer}_{last}"):
            weigh(layer, last, softened)
        pair_copy(layer, last).start()
        with scope(f"own_{layer}_{last}"):
            own_half(hidden, layer, one(last))
        for kind in range(5):
            w_copy(kind, layer + 1).wait()
        for seg in range(segments)[::-1]:
            if seg > 0:
                with scope(f"halo_{layer}_{seg - 1}"):
                    wait_halo(layer, seg - 1)
            with scope(f"pair_{layer}_{seg}"):
                pair_copy(layer, seg).wait_recv()
            with scope(f"block_{layer}_{seg}"):
                if seg > 0:
                    results = scores(layer, seg - 1)
                other_half(layer, one(seg))
                if seg > 0:
                    weigh(layer, seg - 1, soften(results))
                finish(layer, one(seg))
            if seg > 0:
                pair_copy(layer, seg - 1).start()
            with scope(f"kv_{layer}_{seg}"):
                keys_values(following, layer + 1, one(seg))
            with scope(f"own_{layer}_{seg}"):
                if seg > 0:
                    own_half(hidden, layer, one(seg - 1))
                queries_split(following, layer + 1, seg)

    layer, hidden = LAYERS - 1, hiddens[LAYERS - 1]
    late, late_piece = range(2, segments)[::-1], (2, segments)
    with scope("halo_late"):
        for seg in late:
            wait_halo(layer, seg)
    with scope("attend_late"):
        results = [scores(layer, seg) for seg in late]
        for seg, result in zip(late, results):
            weigh(layer, seg, soften(result))
    for seg in late:
        pair_copy(layer, seg).start()
    with scope("own_late"):
        own_half(hidden, layer, late_piece)
    with scope("halo_1"):
        wait_halo(layer, 1)
    with scope("pair_late"):
        for seg in late:
            pair_copy(layer, seg).wait_recv()
    with scope("block_1_late"):
        result = scores(layer, 1)
        other_half(layer, late_piece)
        weigh(layer, 1, soften(result))
        finish(layer, late_piece)
    pair_copy(layer, 1).start()
    with scope("k_0"):
        wait_halo(layer, 0, 0)
    with scope("soften_0_own_1"):
        result = scores(layer, 0)
        own_half(hidden, layer, one(1))
        softened = soften(result)
    with scope("v_0"):
        wait_halo(layer, 0, 1)
    with scope("weigh_0"):
        weigh(layer, 0, softened)
    pair_copy(layer, 0).start()
    with scope("pair_1"):
        pair_copy(layer, 1).wait_recv()
    with scope("finish_1"):
        other_half(layer, one(1))
        own_half(hidden, layer, one(0))
        finish(layer, one(1))
    with scope("pair_0"):
        pair_copy(layer, 0).wait_recv()
    with scope("finish_0"):
        other_half(layer, one(0))
        finish(layer, one(0))

    for layer in range(LAYERS):
        for seg in range(segments):
            pair_copy(layer, seg).wait_send()

    @pl.when(has_next)
    def _():
        for layer in range(LAYERS):
            for seg in range(segments):
                for kind in range(2):
                    halo_copy(kind, layer, seg).wait_send()


def body(
    sp_count, tokens, query_weight, key_weight, value_weight, out_weight, rel_table, norm_gain,
    norm_bias,
):
    rows, model = tokens.shape
    width = query_weight.shape[2]
    heads = rel_table.shape[1]
    reach = LEFT * SEG
    segments = rows // SEG
    wide = -(-(reach + 2 * SEG - 1) // LANES) * LANES
    size = -(-rel_table.shape[2] // LANES) * LANES
    hbm = pl.BlockSpec(memory_space=pltpu.MemorySpace.HBM)
    vmem = pl.BlockSpec(memory_space=pltpu.VMEM)
    bf16 = jnp.bfloat16
    return pl.pallas_call(
        functools.partial(kernel, sp_count, heads),
        out_shape=jax.ShapeDtypeStruct((rows, model // 2), bf16),
        in_specs=[hbm] * 8,
        out_specs=vmem,
        scratch_shapes=[
            pltpu.VMEM((rows, model), bf16),
            pltpu.VMEM((rows, model), bf16),
            pltpu.VMEM(query_weight.shape, bf16),
            pltpu.VMEM(key_weight.shape, bf16),
            pltpu.VMEM(value_weight.shape, bf16),
            pltpu.VMEM((LAYERS, 2, width, model), bf16),
            pltpu.VMEM(rel_table.shape, jnp.float32),
            pltpu.VMEM(norm_gain.shape, jnp.float32),
            pltpu.VMEM(norm_bias.shape, jnp.float32),
            pltpu.VMEM((LAYERS, rows, width), bf16),
            pltpu.VMEM((LAYERS, reach + rows, width), bf16),
            pltpu.VMEM((LAYERS, reach + rows, width), bf16),
            pltpu.VMEM((LAYERS, rows, width), bf16),
            pltpu.VMEM((LAYERS, rows, width), bf16),
            pltpu.VMEM((rows, model), jnp.float32),
            pltpu.VMEM((LAYERS, heads * SEG, wide), jnp.float32),
            pltpu.VMEM((-(-LAYERS * heads // 8) * 8, size), jnp.float32),
            pltpu.SemaphoreType.DMA((2,)),
            pltpu.SemaphoreType.DMA((2, CHUNKS)),
            pltpu.SemaphoreType.DMA((5, LAYERS)),
            pltpu.SemaphoreType.DMA((3,)),
            pltpu.SemaphoreType.DMA((2, LAYERS, segments)),
            pltpu.SemaphoreType.DMA((2, LAYERS, segments)),
            pltpu.SemaphoreType.DMA((LAYERS, segments)),
            pltpu.SemaphoreType.DMA((LAYERS, segments)),
        ],
        compiler_params=pltpu.CompilerParams(
            collective_id=0, has_side_effects=True, vmem_limit_bytes=56000000
        ),
    )(
        *(
            pltpu.with_memory_space_constraint(operand, pltpu.MemorySpace.HBM)
            for operand in (
                tokens,
                query_weight,
                key_weight,
                value_weight,
                out_weight,
                rel_table,
                norm_gain,
                norm_bias,
            )
        )
    )


def solution(mesh):
    return jax.shard_map(
        functools.partial(body, mesh.shape["sp"]),
        mesh=mesh,
        in_specs=(
            P("sp", None),
            P(None, None, "tp"),
            P(None, None, "tp"),
            P(None, None, "tp"),
            P(),
            P(None, "tp", None),
            P(),
            P(),
        ),
        out_specs=P("sp", "tp"),
        check_vma=False,
    )
```

```python
import functools

import jax
import jax.numpy as jnp
from jax import lax
from jax.experimental import pallas as pl
from jax.experimental.pallas import tpu as pltpu
from jax.sharding import PartitionSpec as P

SEG = 64
LEFT = 4
CLIP = 128
LAYERS = 2
LANES = 128
CHUNKS = 4

residual_scale = 2.0**0.5
norm_eps = 1e-05
masked_score = -1e30
MESH = pl.DeviceIdType.MESH


def kernel(
    sp_count,
    heads,
    tokens,
    wq_hbm,
    wk_hbm,
    wv_hbm,
    wo_hbm,
    table_hbm,
    gain_hbm,
    shift_hbm,
    out,
    x0,
    x1,
    wq,
    wk,
    wv,
    wo,
    table,
    gain,
    shift,
    query,
    kx,
    vx,
    att,
    peer,
    total,
    bias,
    padded,
    x_sem,
    first_sem,
    w_sem,
    small_sem,
    halo_send,
    halo_recv,
    pair_send,
    pair_recv,
):
    rows, model = x0.shape
    width = query.shape[2]
    head_size = width // heads
    reach = LEFT * SEG
    band = reach + SEG
    segments = rows // SEG
    sp = lax.axis_index("sp")
    tp = lax.axis_index("tp")
    has_next = sp < sp_count - 1
    has_prev = sp > 0

    def first_copy(kind, index):
        size = model // CHUNKS
        part = pl.ds(index * size, size)
        return pltpu.make_async_copy(
            (wk_hbm, wv_hbm)[kind].at[0, part],
            (wk, wv)[kind].at[0, part],
            first_sem.at[kind, index],
        )

    def w_copy(kind, layer):
        if kind < 3:
            source = (wk_hbm, wv_hbm, wq_hbm)[kind].at[layer]
            target = (wk, wv, wq)[kind].at[layer]
        else:
            owner = (tp, 1 - tp)[kind - 3]
            part = pl.ds(pl.multiple_of(owner * width, width), width)
            source = wo_hbm.at[layer, part]
            target = wo.at[layer, kind - 3]
        return pltpu.make_async_copy(source, target, w_sem.at[kind, layer])

    def x_copy(index, first, count):
        part = pl.ds(first, count)
        return pltpu.make_async_copy(tokens.at[part], x0.at[part], x_sem.at[index])

    x_last = x_copy(0, rows - SEG, SEG)
    x_rest = x_copy(1, 0, rows - SEG)
    small = [
        pltpu.make_async_copy(source, target, small_sem.at[index])
        for index, (source, target) in enumerate(
            ((table_hbm, table), (gain_hbm, gain), (shift_hbm, shift))
        )
    ]

    def halo_copy(kind, layer, seg):
        buffer = (kx, vx)[kind]
        return pltpu.make_async_remote_copy(
            src_ref=buffer.at[layer, pl.ds(reach + seg * SEG, SEG)],
            dst_ref=buffer.at[layer, pl.ds(seg * SEG, SEG)],
            send_sem=halo_send.at[kind, layer, seg],
            recv_sem=halo_recv.at[kind, layer, seg],
            device_id=(jnp.minimum(sp + 1, sp_count - 1), tp),
            device_id_type=MESH,
        )

    def pair_copy(layer, seg):
        part = pl.ds(seg * SEG, SEG)
        return pltpu.make_async_remote_copy(
            src_ref=att.at[layer, part],
            dst_ref=peer.at[layer, part],
            send_sem=pair_send.at[layer, seg],
            recv_sem=pair_recv.at[layer, seg],
            device_id=(sp, 1 - tp),
            device_id_type=MESH,
        )

    barrier = pltpu.get_barrier_semaphore()
    pl.semaphore_signal(barrier, inc=1, device_id=(sp, 1 - tp), device_id_type=MESH)

    @pl.when(has_prev)
    def _():
        pl.semaphore_signal(barrier, inc=1, device_id=(sp - 1, tp), device_id_type=MESH)

    x_last.start()
    first = [first_copy(kind, index) for kind in range(2) for index in range(CHUNKS)]
    for copy in first[:CHUNKS]:
        copy.start()
    pl.delay(200)
    for copy in first[CHUNKS:]:
        copy.start()
    x_rest.start()
    w_copy(2, 0).start()

    @pl.when(jnp.logical_not(has_prev))
    def _():
        for layer in range(LAYERS):
            kx[layer, :reach, :] = jnp.zeros((reach, width), jnp.bfloat16)
            vx[layer, :reach, :] = jnp.zeros((reach, width), jnp.bfloat16)

    def build_bias():
        wide = bias.shape[2]
        size = padded.shape[1]
        padded[...] = jnp.zeros_like(padded)
        for layer in range(LAYERS):
            padded[layer * heads : (layer + 1) * heads, : table.shape[2]] = table[layer]
        place = lax.broadcasted_iota(jnp.int32, (size, wide), 1)
        source = lax.broadcasted_iota(jnp.int32, (size, wide), 0)
        onehot = (jnp.clip(band - 1 - place, -CLIP, CLIP) + CLIP == source).astype(jnp.float32)
        by_offset = jnp.dot(
            padded[...],
            onehot,
            precision=lax.Precision.HIGHEST,
            preferred_element_type=jnp.float32,
        )
        for layer in range(LAYERS):
            for h in range(heads):
                line = by_offset[layer * heads + h : layer * heads + h + 1, :]
                skewed = pltpu.roll(
                    jnp.broadcast_to(line, (SEG, wide)), wide - SEG + 1, 1, stride=1, stride_axis=0
                )
                bias[layer, h * SEG : (h + 1) * SEG, :] = skewed

    def rows_of(piece):
        return slice(piece[0] * SEG, piece[1] * SEG)

    def project(hidden, layer, part, kind):
        weight = (wk, wv, wq)[kind]
        return jnp.dot(
            hidden[part, :], weight[layer], preferred_element_type=jnp.float32
        ).astype(jnp.bfloat16)

    def keys_values(hidden, layer, piece):
        part = rows_of(piece)
        target = slice(reach + part.start, reach + part.stop)
        kx[layer, target, :] = project(hidden, layer, part, 0)
        vx[layer, target, :] = project(hidden, layer, part, 1)

    def send(layer, piece, core):
        @pl.when(has_next & (tp == core))
        def _():
            for seg in range(*piece)[::-1]:
                halo_copy(0, layer, seg).start()
                halo_copy(1, layer, seg).start()

    def project_split(hidden, layer, part, kind):
        weight = (wk, wv, wq)[kind]
        return [
            jnp.dot(
                hidden[part, :],
                weight[layer, :, first : first + LANES],
                preferred_element_type=jnp.float32,
            ).astype(jnp.bfloat16)
            for first in range(0, width, LANES)
        ]

    def store_keys(hidden, layer, seg):
        target = slice(reach + seg * SEG, reach + (seg + 1) * SEG)
        for group, block in enumerate(
            project_split(hidden, layer, slice(seg * SEG, (seg + 1) * SEG), 0)
        ):
            kx[layer, target, group * LANES : (group + 1) * LANES] = block

    def values(hidden, layer, seg):
        target = slice(reach + seg * SEG, reach + (seg + 1) * SEG)
        for group, block in enumerate(
            project_split(hidden, layer, slice(seg * SEG, (seg + 1) * SEG), 1)
        ):
            vx[layer, target, group * LANES : (group + 1) * LANES] = block

        @pl.when(has_next)
        def _():
            halo_copy(1, layer, seg).start()

    def queries_split(hidden, layer, seg):
        part = slice(seg * SEG, (seg + 1) * SEG)
        for group, block in enumerate(project_split(hidden, layer, part, 2)):
            query[layer, part, group * LANES : (group + 1) * LANES] = block * jnp.bfloat16(
                head_size**-0.5
            )

    def queries(hidden, layer, piece):
        first, last = piece[0] * SEG, piece[1] * SEG
        middle = (first + last) // 2 if last - first > SEG else last
        for part in (slice(first, middle), slice(middle, last)):
            if part.start == part.stop:
                continue
            query[layer, part, :] = project(hidden, layer, part, 2) * jnp.bfloat16(
                head_size**-0.5
            )

    def wait_halo(layer, seg, kind=None):
        @pl.when(has_prev)
        def _():
            for each in (0, 1) if kind is None else (kind,):
                halo_copy(each, layer, seg).wait_recv()

    pair = LANES // head_size
    lane = lax.broadcasted_iota(jnp.int32, (1, LANES), 1)
    in_pair = [
        (lane >= h * head_size) & (lane < (h + 1) * head_size) for h in range(pair)
    ]

    def scores(layer, seg):
        column = lax.broadcasted_iota(jnp.int32, (1, band), 1)
        outside = (column < reach - seg * SEG) & jnp.logical_not(has_prev)
        results = []
        for group in range(width // LANES):
            lanes = slice(group * LANES, (group + 1) * LANES)
            block = query[layer, seg * SEG : (seg + 1) * SEG, lanes]
            stacked = jnp.concatenate(
                [jnp.where(in_pair[h], block, jnp.zeros_like(block)) for h in range(pair)], axis=0
            )
            raw = lax.dot_general(
                stacked,
                kx[layer, seg * SEG : seg * SEG + band, lanes],
                (((1,), (1,)), ((), ())),
                preferred_element_type=jnp.float32,
            )
            lines = slice(group * pair * SEG, (group + 1) * pair * SEG)
            results.append(jnp.where(outside, masked_score, raw + bias[layer, lines, :band]))
        return results

    def soften(results):
        softened = []
        for raw in results:
            expo = jnp.exp(raw - jnp.max(raw, -1, keepdims=True))
            norm = jnp.sum(expo, -1, keepdims=True)
            softened.append((expo.astype(jnp.bfloat16), 1.0 / norm))
        return softened

    def weigh(layer, seg, softened):
        for group, (expo, inverse) in enumerate(softened):
            lanes = slice(group * LANES, (group + 1) * LANES)
            mixed = jnp.dot(
                expo,
                vx[layer, seg * SEG : seg * SEG + band, lanes],
                preferred_element_type=jnp.float32,
            )
            mixed = mixed * inverse
            own = mixed[:SEG, :]
            for h in range(1, pair):
                own = jnp.where(in_pair[h], mixed[h * SEG : (h + 1) * SEG, :], own)
            att[layer, seg * SEG : (seg + 1) * SEG, lanes] = own.astype(jnp.bfloat16)

    def half(layer, piece, source, index):
        return jnp.dot(
            source[layer, rows_of(piece), :],
            wo[layer, index],
            preferred_element_type=jnp.float32,
        )

    def own_half(hidden, layer, piece):
        part = rows_of(piece)
        total[part, :] = half(layer, piece, att, 0) + residual_scale * hidden[part, :].astype(
            jnp.float32
        )

    def other_half(layer, piece):
        total[rows_of(piece), :] += half(layer, piece, peer, 1)

    def finish(layer, piece):
        step = 16
        part = rows_of(piece)
        for r in range(part.start, part.stop, step):
            here = slice(r, r + step)
            value = total[here, :]
            mean = jnp.sum(value, -1, keepdims=True) * (1.0 / model)
            centred = value - mean
            variance = jnp.sum(centred * centred, -1, keepdims=True) * (1.0 / model)
            scale = lax.rsqrt(variance + norm_eps)
            if layer < LAYERS - 1:
                x1[here, :] = (
                    centred * scale * gain[layer : layer + 1, :] + shift[layer : layer + 1, :]
                ).astype(jnp.bfloat16)
            else:
                cols = pl.ds(pl.multiple_of(tp * (model // 2), model // 2), model // 2)
                out[here, :] = (
                    (total[here, cols] - mean) * scale * gain[layer : layer + 1, cols]
                    + shift[layer : layer + 1, cols]
                ).astype(jnp.bfloat16)

    last = segments - 1
    scope = jax.named_scope
    with scope("x_last"):
        x_last.wait()
    with scope("w_k"):
        for copy in first[:CHUNKS]:
            copy.wait()
    with scope("k_last"):
        store_keys(x0, 0, last)
    with scope("barrier"):
        pl.semaphore_wait(barrier, 1 + has_next.astype(jnp.int32))

    @pl.when(has_next)
    def _():
        halo_copy(0, 0, last).start()

    with scope("w_v"):
        for copy in first[CHUNKS:]:
            copy.wait()
    with scope("v_last"):
        values(x0, 0, last)
    with scope("x_rest"):
        x_rest.wait()
    for copy in (*small, w_copy(3, 0), w_copy(4, 0)):
        copy.start()
    with scope("kv_next"):
        keys_values(x0, 0, (last - 1, last))
        send(0, (last - 1, last), 0)
    with scope("kv_rest"):
        keys_values(x0, 0, (0, last - 1))
        send(0, (0, last - 1), 0)
    w_copy(2, 0).wait()
    with scope("queries"):
        queries(x0, 0, (0, segments))
    send(0, (0, last), 1)
    for kind in range(5):
        w_copy(kind, 1).start()
    for copy in small:
        copy.wait()
    with scope("bias"):
        build_bias()
    w_copy(3, 0).wait()
    w_copy(4, 0).wait()

    def one(seg):
        return (seg, seg + 1)

    hiddens = (x0, x1)
    for layer in range(LAYERS - 1):
        hidden, following = hiddens[layer], hiddens[layer + 1]
        with scope(f"k_{layer}_{last}"):
            wait_halo(layer, last, 0)
        with scope(f"soften_{layer}_{last}"):
            softened = soften(scores(layer, last))
        with scope(f"v_{layer}_{last}"):
            wait_halo(layer, last, 1)
        with scope(f"weigh_{layer}_{last}"):
            weigh(layer, last, softened)
        pair_copy(layer, last).start()
        with scope(f"own_{layer}_{last}"):
            own_half(hidden, layer, one(last))
        for kind in range(5):
            w_copy(kind, layer + 1).wait()
        for seg in range(segments)[::-1]:
            if seg > 0:
                with scope(f"halo_{layer}_{seg - 1}"):
                    wait_halo(layer, seg - 1)
            with scope(f"pair_{layer}_{seg}"):
                pair_copy(layer, seg).wait_recv()
            with scope(f"block_{layer}_{seg}"):
                if seg > 0:
                    results = scores(layer, seg - 1)
                other_half(layer, one(seg))
                if seg > 0:
                    weigh(layer, seg - 1, soften(results))
                finish(layer, one(seg))
            if seg > 0:
                pair_copy(layer, seg - 1).start()
            with scope(f"kv_{layer}_{seg}"):
                keys_values(following, layer + 1, one(seg))
                send(layer + 1, one(seg), 0)
            with scope(f"own_{layer}_{seg}"):
                if seg > 0:
                    own_half(hidden, layer, one(seg - 1))
                queries_split(following, layer + 1, seg)
                send(layer + 1, one(seg), 1)

    layer, hidden = LAYERS - 1, hiddens[LAYERS - 1]
    late, late_piece = range(2, segments)[::-1], (2, segments)
    with scope("halo_late"):
        for seg in late:
            wait_halo(layer, seg)
    with scope("attend_late"):
        results = [scores(layer, seg) for seg in late]
        for seg, result in zip(late, results):
            weigh(layer, seg, soften(result))
    for seg in late:
        pair_copy(layer, seg).start()
    with scope("own_late"):
        own_half(hidden, layer, late_piece)
    with scope("halo_1"):
        wait_halo(layer, 1)
    with scope("pair_late"):
        for seg in late:
            pair_copy(layer, seg).wait_recv()
    with scope("block_1_late"):
        result = scores(layer, 1)
        other_half(layer, late_piece)
        weigh(layer, 1, soften(result))
        finish(layer, late_piece)
    pair_copy(layer, 1).start()
    with scope("k_0"):
        wait_halo(layer, 0, 0)
    with scope("soften_0_own_1"):
        result = scores(layer, 0)
        own_half(hidden, layer, one(1))
        softened = soften(result)
    with scope("v_0"):
        wait_halo(layer, 0, 1)
    with scope("weigh_0"):
        weigh(layer, 0, softened)
    pair_copy(layer, 0).start()
    with scope("pair_1"):
        pair_copy(layer, 1).wait_recv()
    with scope("finish_1"):
        other_half(layer, one(1))
        own_half(hidden, layer, one(0))
        finish(layer, one(1))
    with scope("pair_0"):
        pair_copy(layer, 0).wait_recv()
    with scope("finish_0"):
        other_half(layer, one(0))
        finish(layer, one(0))

    for layer in range(LAYERS):
        for seg in range(segments):
            pair_copy(layer, seg).wait_send()

    @pl.when(has_next)
    def _():
        for layer in range(LAYERS):
            for seg in range(segments):
                for kind in range(2):
                    halo_copy(kind, layer, seg).wait_send()


def body(
    sp_count, tokens, query_weight, key_weight, value_weight, out_weight, rel_table, norm_gain,
    norm_bias,
):
    rows, model = tokens.shape
    width = query_weight.shape[2]
    heads = rel_table.shape[1]
    reach = LEFT * SEG
    segments = rows // SEG
    wide = -(-(reach + 2 * SEG - 1) // LANES) * LANES
    size = -(-rel_table.shape[2] // LANES) * LANES
    hbm = pl.BlockSpec(memory_space=pltpu.MemorySpace.HBM)
    vmem = pl.BlockSpec(memory_space=pltpu.VMEM)
    bf16 = jnp.bfloat16
    return pl.pallas_call(
        functools.partial(kernel, sp_count, heads),
        out_shape=jax.ShapeDtypeStruct((rows, model // 2), bf16),
        in_specs=[hbm] * 8,
        out_specs=vmem,
        scratch_shapes=[
            pltpu.VMEM((rows, model), bf16),
            pltpu.VMEM((rows, model), bf16),
            pltpu.VMEM(query_weight.shape, bf16),
            pltpu.VMEM(key_weight.shape, bf16),
            pltpu.VMEM(value_weight.shape, bf16),
            pltpu.VMEM((LAYERS, 2, width, model), bf16),
            pltpu.VMEM(rel_table.shape, jnp.float32),
            pltpu.VMEM(norm_gain.shape, jnp.float32),
            pltpu.VMEM(norm_bias.shape, jnp.float32),
            pltpu.VMEM((LAYERS, rows, width), bf16),
            pltpu.VMEM((LAYERS, reach + rows, width), bf16),
            pltpu.VMEM((LAYERS, reach + rows, width), bf16),
            pltpu.VMEM((LAYERS, rows, width), bf16),
            pltpu.VMEM((LAYERS, rows, width), bf16),
            pltpu.VMEM((rows, model), jnp.float32),
            pltpu.VMEM((LAYERS, heads * SEG, wide), jnp.float32),
            pltpu.VMEM((-(-LAYERS * heads // 8) * 8, size), jnp.float32),
            pltpu.SemaphoreType.DMA((2,)),
            pltpu.SemaphoreType.DMA((2, CHUNKS)),
            pltpu.SemaphoreType.DMA((5, LAYERS)),
            pltpu.SemaphoreType.DMA((3,)),
            pltpu.SemaphoreType.DMA((2, LAYERS, segments)),
            pltpu.SemaphoreType.DMA((2, LAYERS, segments)),
            pltpu.SemaphoreType.DMA((LAYERS, segments)),
            pltpu.SemaphoreType.DMA((LAYERS, segments)),
        ],
        compiler_params=pltpu.CompilerParams(
            collective_id=0, has_side_effects=True, vmem_limit_bytes=56000000
        ),
    )(
        *(
            pltpu.with_memory_space_constraint(operand, pltpu.MemorySpace.HBM)
            for operand in (
                tokens,
                query_weight,
                key_weight,
                value_weight,
                out_weight,
                rel_table,
                norm_gain,
                norm_bias,
            )
        )
    )


def solution(mesh):
    return jax.shard_map(
        functools.partial(body, mesh.shape["sp"]),
        mesh=mesh,
        in_specs=(
            P("sp", None),
            P(None, None, "tp"),
            P(None, None, "tp"),
            P(None, None, "tp"),
            P(),
            P(None, "tp", None),
            P(),
            P(),
        ),
        out_specs=P("sp", "tp"),
        check_vma=False,
    )
```

```python
import functools

import jax
import jax.numpy as jnp
from jax import lax
from jax.experimental import pallas as pl
from jax.experimental.pallas import tpu as pltpu
from jax.sharding import PartitionSpec as P

SEG = 64
LEFT = 4
CLIP = 128
LAYERS = 2
LANES = 128
CHUNKS = 4

residual_scale = 2.0**0.5
norm_eps = 1e-05
masked_score = -1e30
MESH = pl.DeviceIdType.MESH


def kernel(
    sp_count,
    heads,
    tokens,
    wq_hbm,
    wk_hbm,
    wv_hbm,
    wo_hbm,
    table_hbm,
    gain_hbm,
    shift_hbm,
    out,
    x0,
    x1,
    wq,
    wk,
    wv,
    wo,
    table,
    gain,
    shift,
    query,
    kx,
    vx,
    att,
    peer,
    total,
    bias,
    padded,
    x_sem,
    first_sem,
    w_sem,
    small_sem,
    halo_send,
    halo_recv,
    pair_send,
    pair_recv,
):
    rows, model = x0.shape
    width = query.shape[2]
    head_size = width // heads
    reach = LEFT * SEG
    band = reach + SEG
    segments = rows // SEG
    sp = lax.axis_index("sp")
    tp = lax.axis_index("tp")
    has_next = sp < sp_count - 1
    has_prev = sp > 0

    def first_copy(kind, index):
        size = model // CHUNKS
        part = pl.ds(index * size, size)
        return pltpu.make_async_copy(
            (wk_hbm, wv_hbm)[kind].at[0, part],
            (wk, wv)[kind].at[0, part],
            first_sem.at[kind, index],
        )

    def w_copy(kind, layer):
        if kind < 3:
            source = (wk_hbm, wv_hbm, wq_hbm)[kind].at[layer]
            target = (wk, wv, wq)[kind].at[layer]
        else:
            owner = (tp, 1 - tp)[kind - 3]
            part = pl.ds(pl.multiple_of(owner * width, width), width)
            source = wo_hbm.at[layer, part]
            target = wo.at[layer, kind - 3]
        return pltpu.make_async_copy(source, target, w_sem.at[kind, layer])

    def x_copy(index, first, count):
        part = pl.ds(first, count)
        return pltpu.make_async_copy(tokens.at[part], x0.at[part], x_sem.at[index])

    x_last = x_copy(0, rows - SEG, SEG)
    x_rest = x_copy(1, 0, rows - SEG)
    small = [
        pltpu.make_async_copy(source, target, small_sem.at[index])
        for index, (source, target) in enumerate(
            ((table_hbm, table), (gain_hbm, gain), (shift_hbm, shift))
        )
    ]

    def halo_copy(kind, layer, seg):
        buffer = (kx, vx)[kind]
        return pltpu.make_async_remote_copy(
            src_ref=buffer.at[layer, pl.ds(reach + seg * SEG, SEG)],
            dst_ref=buffer.at[layer, pl.ds(seg * SEG, SEG)],
            send_sem=halo_send.at[kind, layer, seg],
            recv_sem=halo_recv.at[kind, layer, seg],
            device_id=(jnp.minimum(sp + 1, sp_count - 1), tp),
            device_id_type=MESH,
        )

    def pair_copy(layer, seg):
        part = pl.ds(seg * SEG, SEG)
        return pltpu.make_async_remote_copy(
            src_ref=att.at[layer, part],
            dst_ref=peer.at[layer, part],
            send_sem=pair_send.at[layer, seg],
            recv_sem=pair_recv.at[layer, seg],
            device_id=(sp, 1 - tp),
            device_id_type=MESH,
        )

    barrier = pltpu.get_barrier_semaphore()
    pl.semaphore_signal(barrier, inc=1, device_id=(sp, 1 - tp), device_id_type=MESH)

    @pl.when(has_prev)
    def _():
        pl.semaphore_signal(barrier, inc=1, device_id=(sp - 1, tp), device_id_type=MESH)

    x_last.start()
    first = [first_copy(kind, index) for kind in range(2) for index in range(CHUNKS)]
    for copy in first[:CHUNKS]:
        copy.start()
    pl.delay(200)
    for copy in first[CHUNKS:]:
        copy.start()
    x_rest.start()
    w_copy(2, 0).start()

    @pl.when(jnp.logical_not(has_prev))
    def _():
        for layer in range(LAYERS):
            kx[layer, :reach, :] = jnp.zeros((reach, width), jnp.bfloat16)
            vx[layer, :reach, :] = jnp.zeros((reach, width), jnp.bfloat16)

    def build_bias():
        wide = bias.shape[2]
        size = padded.shape[1]
        padded[...] = jnp.zeros_like(padded)
        for layer in range(LAYERS):
            padded[layer * heads : (layer + 1) * heads, : table.shape[2]] = table[layer]
        place = lax.broadcasted_iota(jnp.int32, (size, wide), 1)
        source = lax.broadcasted_iota(jnp.int32, (size, wide), 0)
        onehot = (jnp.clip(band - 1 - place, -CLIP, CLIP) + CLIP == source).astype(jnp.float32)
        by_offset = jnp.dot(
            padded[...],
            onehot,
            precision=lax.Precision.HIGHEST,
            preferred_element_type=jnp.float32,
        )
        for layer in range(LAYERS):
            for h in range(heads):
                line = by_offset[layer * heads + h : layer * heads + h + 1, :]
                skewed = pltpu.roll(
                    jnp.broadcast_to(line, (SEG, wide)), wide - SEG + 1, 1, stride=1, stride_axis=0
                )
                bias[layer, h * SEG : (h + 1) * SEG, :] = skewed

    def rows_of(piece):
        return slice(piece[0] * SEG, piece[1] * SEG)

    def project(hidden, layer, part, kind):
        weight = (wk, wv, wq)[kind]
        return jnp.dot(
            hidden[part, :], weight[layer], preferred_element_type=jnp.float32
        ).astype(jnp.bfloat16)

    def keys_values(hidden, layer, piece):
        part = rows_of(piece)
        target = slice(reach + part.start, reach + part.stop)
        kx[layer, target, :] = project(hidden, layer, part, 0)
        vx[layer, target, :] = project(hidden, layer, part, 1)

    def send(layer, piece, core):
        @pl.when(has_next & (tp == core))
        def _():
            for seg in range(*piece)[::-1]:
                halo_copy(0, layer, seg).start()
                halo_copy(1, layer, seg).start()

    def project_split(hidden, layer, part, kind):
        weight = (wk, wv, wq)[kind]
        return [
            jnp.dot(
                hidden[part, :],
                weight[layer, :, first : first + LANES],
                preferred_element_type=jnp.float32,
            ).astype(jnp.bfloat16)
            for first in range(0, width, LANES)
        ]

    def store_keys(hidden, layer, seg):
        target = slice(reach + seg * SEG, reach + (seg + 1) * SEG)
        for group, block in enumerate(
            project_split(hidden, layer, slice(seg * SEG, (seg + 1) * SEG), 0)
        ):
            kx[layer, target, group * LANES : (group + 1) * LANES] = block

    def values(hidden, layer, seg):
        target = slice(reach + seg * SEG, reach + (seg + 1) * SEG)
        for group, block in enumerate(
            project_split(hidden, layer, slice(seg * SEG, (seg + 1) * SEG), 1)
        ):
            vx[layer, target, group * LANES : (group + 1) * LANES] = block

        @pl.when(has_next)
        def _():
            halo_copy(1, layer, seg).start()

    def queries_split(hidden, layer, seg):
        part = slice(seg * SEG, (seg + 1) * SEG)
        for group, block in enumerate(project_split(hidden, layer, part, 2)):
            query[layer, part, group * LANES : (group + 1) * LANES] = block * jnp.bfloat16(
                head_size**-0.5
            )

    def queries(hidden, layer, piece):
        first, last = piece[0] * SEG, piece[1] * SEG
        middle = (first + last) // 2 if last - first > SEG else last
        for part in (slice(first, middle), slice(middle, last)):
            if part.start == part.stop:
                continue
            query[layer, part, :] = project(hidden, layer, part, 2) * jnp.bfloat16(
                head_size**-0.5
            )

    def wait_halo(layer, seg, kind=None):
        @pl.when(has_prev)
        def _():
            for each in (0, 1) if kind is None else (kind,):
                halo_copy(each, layer, seg).wait_recv()

    pair = LANES // head_size
    lane = lax.broadcasted_iota(jnp.int32, (1, LANES), 1)
    in_pair = [
        (lane >= h * head_size) & (lane < (h + 1) * head_size) for h in range(pair)
    ]

    def scores(layer, seg):
        column = lax.broadcasted_iota(jnp.int32, (1, band), 1)
        outside = (column < reach - seg * SEG) & jnp.logical_not(has_prev)
        results = []
        for group in range(width // LANES):
            lanes = slice(group * LANES, (group + 1) * LANES)
            block = query[layer, seg * SEG : (seg + 1) * SEG, lanes]
            stacked = jnp.concatenate(
                [jnp.where(in_pair[h], block, jnp.zeros_like(block)) for h in range(pair)], axis=0
            )
            raw = lax.dot_general(
                stacked,
                kx[layer, seg * SEG : seg * SEG + band, lanes],
                (((1,), (1,)), ((), ())),
                preferred_element_type=jnp.float32,
            )
            lines = slice(group * pair * SEG, (group + 1) * pair * SEG)
            results.append(jnp.where(outside, masked_score, raw + bias[layer, lines, :band]))
        return results

    def soften(results):
        softened = []
        for raw in results:
            expo = jnp.exp(raw - jnp.max(raw, -1, keepdims=True))
            norm = jnp.sum(expo, -1, keepdims=True)
            softened.append((expo.astype(jnp.bfloat16), 1.0 / norm))
        return softened

    def weigh(layer, seg, softened):
        for group, (expo, inverse) in enumerate(softened):
            lanes = slice(group * LANES, (group + 1) * LANES)
            mixed = jnp.dot(
                expo,
                vx[layer, seg * SEG : seg * SEG + band, lanes],
                preferred_element_type=jnp.float32,
            )
            mixed = mixed * inverse
            own = mixed[:SEG, :]
            for h in range(1, pair):
                own = jnp.where(in_pair[h], mixed[h * SEG : (h + 1) * SEG, :], own)
            att[layer, seg * SEG : (seg + 1) * SEG, lanes] = own.astype(jnp.bfloat16)

    def half(layer, piece, source, index):
        return jnp.dot(
            source[layer, rows_of(piece), :],
            wo[layer, index],
            preferred_element_type=jnp.float32,
        )

    def own_half(hidden, layer, piece):
        part = rows_of(piece)
        total[part, :] = half(layer, piece, att, 0) + residual_scale * hidden[part, :].astype(
            jnp.float32
        )

    def other_half(layer, piece):
        total[rows_of(piece), :] += half(layer, piece, peer, 1)

    def finish(layer, piece):
        step = 16
        part = rows_of(piece)
        for r in range(part.start, part.stop, step):
            here = slice(r, r + step)
            value = total[here, :]
            mean = jnp.sum(value, -1, keepdims=True) * (1.0 / model)
            centred = value - mean
            variance = jnp.sum(centred * centred, -1, keepdims=True) * (1.0 / model)
            scale = lax.rsqrt(variance + norm_eps)
            if layer < LAYERS - 1:
                x1[here, :] = (
                    centred * scale * gain[layer : layer + 1, :] + shift[layer : layer + 1, :]
                ).astype(jnp.bfloat16)
            else:
                cols = pl.ds(pl.multiple_of(tp * (model // 2), model // 2), model // 2)
                out[here, :] = (
                    (total[here, cols] - mean) * scale * gain[layer : layer + 1, cols]
                    + shift[layer : layer + 1, cols]
                ).astype(jnp.bfloat16)

    last = segments - 1
    scope = jax.named_scope
    with scope("x_last"):
        x_last.wait()
    with scope("w_k"):
        for copy in first[:CHUNKS]:
            copy.wait()
    with scope("k_last"):
        store_keys(x0, 0, last)
    with scope("barrier"):
        pl.semaphore_wait(barrier, 1 + has_next.astype(jnp.int32))

    @pl.when(has_next)
    def _():
        halo_copy(0, 0, last).start()

    with scope("w_v"):
        for copy in first[CHUNKS:]:
            copy.wait()
    with scope("v_last"):
        values(x0, 0, last)
    with scope("x_rest"):
        x_rest.wait()
    for copy in (*small, w_copy(3, 0), w_copy(4, 0)):
        copy.start()
    with scope("kv_next"):
        keys_values(x0, 0, (last - 1, last))
        send(0, (last - 1, last), 0)
    with scope("kv_rest"):
        keys_values(x0, 0, (0, last - 1))
        send(0, (0, last - 1), 0)
    w_copy(2, 0).wait()
    for kind in range(2):
        w_copy(kind, 1).start()
    with scope("queries"):
        queries(x0, 0, (0, segments))
    send(0, (0, last), 1)
    for copy in small:
        copy.wait()
    with scope("bias"):
        build_bias()
    for kind in range(2, 5):
        w_copy(kind, 1).start()
    w_copy(3, 0).wait()
    w_copy(4, 0).wait()

    def one(seg):
        return (seg, seg + 1)

    hiddens = (x0, x1)
    for layer in range(LAYERS - 1):
        hidden, following = hiddens[layer], hiddens[layer + 1]
        with scope(f"k_{layer}_{last}"):
            wait_halo(layer, last, 0)
        with scope(f"soften_{layer}_{last}"):
            softened = soften(scores(layer, last))
        with scope(f"v_{layer}_{last}"):
            wait_halo(layer, last, 1)
        with scope(f"weigh_{layer}_{last}"):
            weigh(layer, last, softened)
        pair_copy(layer, last).start()
        with scope(f"own_{layer}_{last}"):
            own_half(hidden, layer, one(last))
        for seg in range(segments)[::-1]:
            if seg > 0:
                with scope(f"halo_{layer}_{seg - 1}"):
                    wait_halo(layer, seg - 1)
            with scope(f"pair_{layer}_{seg}"):
                pair_copy(layer, seg).wait_recv()
            if seg == last:
                with scope(f"w_{layer}"):
                    for kind in range(3):
                        w_copy(kind, layer + 1).wait()
            with scope(f"block_{layer}_{seg}"):
                if seg > 0:
                    results = scores(layer, seg - 1)
                other_half(layer, one(seg))
                if seg > 0:
                    weigh(layer, seg - 1, soften(results))
            if seg > 0:
                pair_copy(layer, seg - 1).start()
            with scope(f"kv_{layer}_{seg}"):
                if seg > 0:
                    own_half(hidden, layer, one(seg - 1))
                finish(layer, one(seg))
                keys_values(following, layer + 1, one(seg))
                if seg > 0:
                    queries_split(following, layer + 1, seg)
                send(layer + 1, one(seg), 0)
                if seg > 0:
                    send(layer + 1, one(seg), 1)
            if seg == 0:
                with scope(f"q_{layer}_{seg}"):
                    queries_split(following, layer + 1, seg)
                    send(layer + 1, one(seg), 1)

    layer, hidden = LAYERS - 1, hiddens[LAYERS - 1]
    w_copy(3, layer).wait()
    w_copy(4, layer).wait()
    late, late_piece = range(2, segments)[::-1], (2, segments)
    with scope("halo_late"):
        for seg in late:
            wait_halo(layer, seg)
    with scope("attend_late"):
        results = [scores(layer, seg) for seg in late]
        for seg, result in zip(late, results):
            weigh(layer, seg, soften(result))
    for seg in late:
        pair_copy(layer, seg).start()
    with scope("own_late"):
        own_half(hidden, layer, late_piece)
    with scope("halo_1"):
        wait_halo(layer, 1)
    with scope("pair_late"):
        for seg in late:
            pair_copy(layer, seg).wait_recv()
    with scope("block_1_late"):
        result = scores(layer, 1)
        other_half(layer, late_piece)
        weigh(layer, 1, soften(result))
        finish(layer, late_piece)
    pair_copy(layer, 1).start()
    with scope("k_0"):
        wait_halo(layer, 0, 0)
    with scope("soften_0_own_1"):
        result = scores(layer, 0)
        own_half(hidden, layer, one(1))
        softened = soften(result)
    with scope("v_0"):
        wait_halo(layer, 0, 1)
    with scope("weigh_0"):
        weigh(layer, 0, softened)
    pair_copy(layer, 0).start()
    with scope("pair_1"):
        pair_copy(layer, 1).wait_recv()
    with scope("finish_1"):
        other_half(layer, one(1))
        own_half(hidden, layer, one(0))
        finish(layer, one(1))
    with scope("pair_0"):
        pair_copy(layer, 0).wait_recv()
    with scope("finish_0"):
        other_half(layer, one(0))
        finish(layer, one(0))

    for layer in range(LAYERS):
        for seg in range(segments):
            pair_copy(layer, seg).wait_send()

    @pl.when(has_next)
    def _():
        for layer in range(LAYERS):
            for seg in range(segments):
                for kind in range(2):
                    halo_copy(kind, layer, seg).wait_send()


def body(
    sp_count, tokens, query_weight, key_weight, value_weight, out_weight, rel_table, norm_gain,
    norm_bias,
):
    rows, model = tokens.shape
    width = query_weight.shape[2]
    heads = rel_table.shape[1]
    reach = LEFT * SEG
    segments = rows // SEG
    wide = -(-(reach + 2 * SEG - 1) // LANES) * LANES
    size = -(-rel_table.shape[2] // LANES) * LANES
    hbm = pl.BlockSpec(memory_space=pltpu.MemorySpace.HBM)
    vmem = pl.BlockSpec(memory_space=pltpu.VMEM)
    bf16 = jnp.bfloat16
    return pl.pallas_call(
        functools.partial(kernel, sp_count, heads),
        out_shape=jax.ShapeDtypeStruct((rows, model // 2), bf16),
        in_specs=[hbm] * 8,
        out_specs=vmem,
        scratch_shapes=[
            pltpu.VMEM((rows, model), bf16),
            pltpu.VMEM((rows, model), bf16),
            pltpu.VMEM(query_weight.shape, bf16),
            pltpu.VMEM(key_weight.shape, bf16),
            pltpu.VMEM(value_weight.shape, bf16),
            pltpu.VMEM((LAYERS, 2, width, model), bf16),
            pltpu.VMEM(rel_table.shape, jnp.float32),
            pltpu.VMEM(norm_gain.shape, jnp.float32),
            pltpu.VMEM(norm_bias.shape, jnp.float32),
            pltpu.VMEM((LAYERS, rows, width), bf16),
            pltpu.VMEM((LAYERS, reach + rows, width), bf16),
            pltpu.VMEM((LAYERS, reach + rows, width), bf16),
            pltpu.VMEM((LAYERS, rows, width), bf16),
            pltpu.VMEM((LAYERS, rows, width), bf16),
            pltpu.VMEM((rows, model), jnp.float32),
            pltpu.VMEM((LAYERS, heads * SEG, wide), jnp.float32),
            pltpu.VMEM((-(-LAYERS * heads // 8) * 8, size), jnp.float32),
            pltpu.SemaphoreType.DMA((2,)),
            pltpu.SemaphoreType.DMA((2, CHUNKS)),
            pltpu.SemaphoreType.DMA((5, LAYERS)),
            pltpu.SemaphoreType.DMA((3,)),
            pltpu.SemaphoreType.DMA((2, LAYERS, segments)),
            pltpu.SemaphoreType.DMA((2, LAYERS, segments)),
            pltpu.SemaphoreType.DMA((LAYERS, segments)),
            pltpu.SemaphoreType.DMA((LAYERS, segments)),
        ],
        compiler_params=pltpu.CompilerParams(
            collective_id=0, has_side_effects=True, vmem_limit_bytes=56000000
        ),
    )(
        *(
            pltpu.with_memory_space_constraint(operand, pltpu.MemorySpace.HBM)
            for operand in (
                tokens,
                query_weight,
                key_weight,
                value_weight,
                out_weight,
                rel_table,
                norm_gain,
                norm_bias,
            )
        )
    )


def solution(mesh):
    return jax.shard_map(
        functools.partial(body, mesh.shape["sp"]),
        mesh=mesh,
        in_specs=(
            P("sp", None),
            P(None, None, "tp"),
            P(None, None, "tp"),
            P(None, None, "tp"),
            P(),
            P(None, "tp", None),
            P(),
            P(),
        ),
        out_specs=P("sp", "tp"),
        check_vma=False,
    )
```

```python
import functools

import jax
import jax.numpy as jnp
from jax import lax
from jax.experimental import pallas as pl
from jax.experimental.pallas import tpu as pltpu
from jax.sharding import PartitionSpec as P

SEG = 64
LEFT = 4
CLIP = 128
LAYERS = 2
LANES = 128
CHUNKS = 4

residual_scale = 2.0**0.5
norm_eps = 1e-05
masked_score = -1e30
MESH = pl.DeviceIdType.MESH


def kernel(
    sp_count,
    heads,
    tokens,
    wq_hbm,
    wk_hbm,
    wv_hbm,
    wo_hbm,
    table_hbm,
    gain_hbm,
    shift_hbm,
    out,
    x0,
    x1,
    wq,
    wk,
    wv,
    wo,
    table,
    gain,
    shift,
    query,
    kx,
    vx,
    att,
    peer,
    total,
    bias,
    padded,
    x_sem,
    first_sem,
    w_sem,
    small_sem,
    halo_send,
    halo_recv,
    pair_send,
    pair_recv,
):
    rows, model = x0.shape
    width = query.shape[2]
    head_size = width // heads
    reach = LEFT * SEG
    band = reach + SEG
    segments = rows // SEG
    sp = lax.axis_index("sp")
    tp = lax.axis_index("tp")
    has_next = sp < sp_count - 1
    has_prev = sp > 0

    def first_copy(kind, index):
        size = model // CHUNKS
        part = pl.ds(index * size, size)
        return pltpu.make_async_copy(
            (wk_hbm, wv_hbm)[kind].at[0, part],
            (wk, wv)[kind].at[0, part],
            first_sem.at[kind, index],
        )

    def w_copy(kind, layer):
        if kind < 3:
            source = (wk_hbm, wv_hbm, wq_hbm)[kind].at[layer]
            target = (wk, wv, wq)[kind].at[layer]
        else:
            owner = (tp, 1 - tp)[kind - 3]
            part = pl.ds(pl.multiple_of(owner * width, width), width)
            source = wo_hbm.at[layer, part]
            target = wo.at[layer, kind - 3]
        return pltpu.make_async_copy(source, target, w_sem.at[kind, layer])

    def x_copy(index, first, count):
        part = pl.ds(first, count)
        return pltpu.make_async_copy(tokens.at[part], x0.at[part], x_sem.at[index])

    x_last = x_copy(0, rows - SEG, SEG)
    x_rest = x_copy(1, 0, rows - SEG)
    small = [
        pltpu.make_async_copy(source, target, small_sem.at[index])
        for index, (source, target) in enumerate(
            ((table_hbm, table), (gain_hbm, gain), (shift_hbm, shift))
        )
    ]

    def halo_copy(kind, layer, seg):
        buffer = (kx, vx)[kind]
        return pltpu.make_async_remote_copy(
            src_ref=buffer.at[layer, pl.ds(reach + seg * SEG, SEG)],
            dst_ref=buffer.at[layer, pl.ds(seg * SEG, SEG)],
            send_sem=halo_send.at[kind, layer, seg],
            recv_sem=halo_recv.at[kind, layer, seg],
            device_id=(jnp.minimum(sp + 1, sp_count - 1), tp),
            device_id_type=MESH,
        )

    def pair_copy(layer, seg):
        part = pl.ds(seg * SEG, SEG)
        return pltpu.make_async_remote_copy(
            src_ref=att.at[layer, part],
            dst_ref=peer.at[layer, part],
            send_sem=pair_send.at[layer, seg],
            recv_sem=pair_recv.at[layer, seg],
            device_id=(sp, 1 - tp),
            device_id_type=MESH,
        )

    barrier = pltpu.get_barrier_semaphore()
    pl.semaphore_signal(barrier, inc=1, device_id=(sp, 1 - tp), device_id_type=MESH)

    @pl.when(has_prev)
    def _():
        pl.semaphore_signal(barrier, inc=1, device_id=(sp - 1, tp), device_id_type=MESH)

    x_last.start()
    first = [first_copy(kind, index) for kind in range(2) for index in range(CHUNKS)]
    for copy in first[:CHUNKS]:
        copy.start()
    pl.delay(200)
    for copy in first[CHUNKS:]:
        copy.start()
    x_rest.start()
    w_copy(2, 0).start()

    @pl.when(jnp.logical_not(has_prev))
    def _():
        for layer in range(LAYERS):
            kx[layer, :reach, :] = jnp.zeros((reach, width), jnp.bfloat16)
            vx[layer, :reach, :] = jnp.zeros((reach, width), jnp.bfloat16)

    def build_bias():
        wide = bias.shape[2]
        size = padded.shape[1]
        padded[...] = jnp.zeros_like(padded)
        for layer in range(LAYERS):
            padded[layer * heads : (layer + 1) * heads, : table.shape[2]] = table[layer]
        place = lax.broadcasted_iota(jnp.int32, (size, wide), 1)
        source = lax.broadcasted_iota(jnp.int32, (size, wide), 0)
        onehot = (jnp.clip(band - 1 - place, -CLIP, CLIP) + CLIP == source).astype(jnp.float32)
        by_offset = jnp.dot(
            padded[...],
            onehot,
            precision=lax.Precision.HIGHEST,
            preferred_element_type=jnp.float32,
        )
        for layer in range(LAYERS):
            for h in range(heads):
                line = by_offset[layer * heads + h : layer * heads + h + 1, :]
                skewed = pltpu.roll(
                    jnp.broadcast_to(line, (SEG, wide)), wide - SEG + 1, 1, stride=1, stride_axis=0
                )
                bias[layer, h * SEG : (h + 1) * SEG, :] = skewed

    def rows_of(piece):
        return slice(piece[0] * SEG, piece[1] * SEG)

    def project(hidden, layer, part, kind):
        weight = (wk, wv, wq)[kind]
        return jnp.dot(
            hidden[part, :], weight[layer], preferred_element_type=jnp.float32
        ).astype(jnp.bfloat16)

    def keys_values(hidden, layer, piece):
        part = rows_of(piece)
        target = slice(reach + part.start, reach + part.stop)
        kx[layer, target, :] = project(hidden, layer, part, 0)
        vx[layer, target, :] = project(hidden, layer, part, 1)

    def send(layer, piece, core):
        @pl.when(has_next & (tp == core))
        def _():
            for seg in range(*piece)[::-1]:
                halo_copy(0, layer, seg).start()
                halo_copy(1, layer, seg).start()

    def project_split(hidden, layer, part, kind):
        weight = (wk, wv, wq)[kind]
        return [
            jnp.dot(
                hidden[part, :],
                weight[layer, :, first : first + LANES],
                preferred_element_type=jnp.float32,
            ).astype(jnp.bfloat16)
            for first in range(0, width, LANES)
        ]

    def store_keys(hidden, layer, seg):
        target = slice(reach + seg * SEG, reach + (seg + 1) * SEG)
        for group, block in enumerate(
            project_split(hidden, layer, slice(seg * SEG, (seg + 1) * SEG), 0)
        ):
            kx[layer, target, group * LANES : (group + 1) * LANES] = block

    def values(hidden, layer, seg):
        target = slice(reach + seg * SEG, reach + (seg + 1) * SEG)
        for group, block in enumerate(
            project_split(hidden, layer, slice(seg * SEG, (seg + 1) * SEG), 1)
        ):
            vx[layer, target, group * LANES : (group + 1) * LANES] = block

        @pl.when(has_next)
        def _():
            halo_copy(1, layer, seg).start()

    def queries_split(hidden, layer, seg):
        part = slice(seg * SEG, (seg + 1) * SEG)
        for group, block in enumerate(project_split(hidden, layer, part, 2)):
            query[layer, part, group * LANES : (group + 1) * LANES] = block * jnp.bfloat16(
                head_size**-0.5
            )

    def queries(hidden, layer, piece):
        first, last = piece[0] * SEG, piece[1] * SEG
        middle = (first + last) // 2 if last - first > SEG else last
        for part in (slice(first, middle), slice(middle, last)):
            if part.start == part.stop:
                continue
            query[layer, part, :] = project(hidden, layer, part, 2) * jnp.bfloat16(
                head_size**-0.5
            )

    def wait_halo(layer, seg, kind=None):
        @pl.when(has_prev)
        def _():
            for each in (0, 1) if kind is None else (kind,):
                halo_copy(each, layer, seg).wait_recv()

    pair = LANES // head_size
    lane = lax.broadcasted_iota(jnp.int32, (1, LANES), 1)
    in_pair = [
        (lane >= h * head_size) & (lane < (h + 1) * head_size) for h in range(pair)
    ]

    def scores(layer, seg):
        column = lax.broadcasted_iota(jnp.int32, (1, band), 1)
        outside = (column < reach - seg * SEG) & jnp.logical_not(has_prev)
        results = []
        for group in range(width // LANES):
            lanes = slice(group * LANES, (group + 1) * LANES)
            block = query[layer, seg * SEG : (seg + 1) * SEG, lanes]
            stacked = jnp.concatenate(
                [jnp.where(in_pair[h], block, jnp.zeros_like(block)) for h in range(pair)], axis=0
            )
            raw = lax.dot_general(
                stacked,
                kx[layer, seg * SEG : seg * SEG + band, lanes],
                (((1,), (1,)), ((), ())),
                preferred_element_type=jnp.float32,
            )
            lines = slice(group * pair * SEG, (group + 1) * pair * SEG)
            results.append(jnp.where(outside, masked_score, raw + bias[layer, lines, :band]))
        return results

    def soften(results):
        softened = []
        for raw in results:
            expo = jnp.exp(raw - jnp.max(raw, -1, keepdims=True))
            norm = jnp.sum(expo, -1, keepdims=True)
            softened.append((expo.astype(jnp.bfloat16), 1.0 / norm))
        return softened

    def weigh(layer, seg, softened):
        for group, (expo, inverse) in enumerate(softened):
            lanes = slice(group * LANES, (group + 1) * LANES)
            mixed = jnp.dot(
                expo,
                vx[layer, seg * SEG : seg * SEG + band, lanes],
                preferred_element_type=jnp.float32,
            )
            mixed = mixed * inverse
            own = mixed[:SEG, :]
            for h in range(1, pair):
                own = jnp.where(in_pair[h], mixed[h * SEG : (h + 1) * SEG, :], own)
            att[layer, seg * SEG : (seg + 1) * SEG, lanes] = own.astype(jnp.bfloat16)

    def half(layer, piece, source, index):
        return jnp.dot(
            source[layer, rows_of(piece), :],
            wo[layer, index],
            preferred_element_type=jnp.float32,
        )

    def own_half(hidden, layer, piece):
        part = rows_of(piece)
        total[part, :] = half(layer, piece, att, 0) + residual_scale * hidden[part, :].astype(
            jnp.float32
        )

    def other_half(layer, piece):
        total[rows_of(piece), :] += half(layer, piece, peer, 1)

    def finish(layer, piece):
        step = 16
        part = rows_of(piece)
        for r in range(part.start, part.stop, step):
            here = slice(r, r + step)
            value = total[here, :]
            mean = jnp.sum(value, -1, keepdims=True) * (1.0 / model)
            centred = value - mean
            variance = jnp.sum(centred * centred, -1, keepdims=True) * (1.0 / model)
            scale = lax.rsqrt(variance + norm_eps)
            if layer < LAYERS - 1:
                x1[here, :] = (
                    centred * scale * gain[layer : layer + 1, :] + shift[layer : layer + 1, :]
                ).astype(jnp.bfloat16)
            else:
                cols = pl.ds(pl.multiple_of(tp * (model // 2), model // 2), model // 2)
                out[here, :] = (
                    (total[here, cols] - mean) * scale * gain[layer : layer + 1, cols]
                    + shift[layer : layer + 1, cols]
                ).astype(jnp.bfloat16)

    last = segments - 1
    scope = jax.named_scope
    with scope("x_last"):
        x_last.wait()
    with scope("w_k"):
        for copy in first[:CHUNKS]:
            copy.wait()
    with scope("k_last"):
        store_keys(x0, 0, last)
    with scope("barrier"):
        pl.semaphore_wait(barrier, 1 + has_next.astype(jnp.int32))

    @pl.when(has_next)
    def _():
        halo_copy(0, 0, last).start()

    with scope("w_v"):
        for copy in first[CHUNKS:]:
            copy.wait()
    with scope("v_last"):
        values(x0, 0, last)
    with scope("x_rest"):
        x_rest.wait()
    for copy in (*small, w_copy(3, 0), w_copy(4, 0)):
        copy.start()
    with scope("kv_next"):
        keys_values(x0, 0, (last - 1, last))
        send(0, (last - 1, last), 0)
    with scope("kv_rest"):
        keys_values(x0, 0, (0, last - 1))
        send(0, (0, last - 1), 0)
    w_copy(2, 0).wait()
    for kind in range(2):
        w_copy(kind, 1).start()
    with scope("queries"):
        queries(x0, 0, (0, segments))
    send(0, (0, last), 1)
    for copy in small:
        copy.wait()
    with scope("bias"):
        build_bias()
    for kind in range(2, 5):
        w_copy(kind, 1).start()
    w_copy(3, 0).wait()
    w_copy(4, 0).wait()

    def one(seg):
        return (seg, seg + 1)

    hiddens = (x0, x1)
    for layer in range(LAYERS - 1):
        hidden, following = hiddens[layer], hiddens[layer + 1]
        with scope(f"k_{layer}_{last}"):
            wait_halo(layer, last, 0)
        with scope(f"soften_{layer}_{last}"):
            softened = soften(scores(layer, last))
        with scope(f"v_{layer}_{last}"):
            wait_halo(layer, last, 1)
        with scope(f"weigh_{layer}_{last}"):
            weigh(layer, last, softened)
        pair_copy(layer, last).start()
        with scope(f"own_{layer}_{last}"):
            own_half(hidden, layer, one(last))
        for seg in range(segments)[::-1]:
            if seg > 0:
                with scope(f"halo_{layer}_{seg - 1}"):
                    wait_halo(layer, seg - 1)
            with scope(f"pair_{layer}_{seg}"):
                pair_copy(layer, seg).wait_recv()
            if seg == last:
                with scope(f"w_{layer}"):
                    for kind in range(3):
                        w_copy(kind, layer + 1).wait()
            with scope(f"block_{layer}_{seg}"):
                if seg > 0:
                    results = scores(layer, seg - 1)
                other_half(layer, one(seg))
                if seg > 0:
                    weigh(layer, seg - 1, soften(results))
            if seg > 0:
                pair_copy(layer, seg - 1).start()
            with scope(f"kv_{layer}_{seg}"):
                if seg > 0:
                    own_half(hidden, layer, one(seg - 1))
                finish(layer, one(seg))
                keys_values(following, layer + 1, one(seg))
                send(layer + 1, one(seg), 0)
                if seg > 0:
                    send(layer + 1, one(seg), 1)
            if seg == 0:
                with scope(f"q_{layer}_{seg}"):
                    send(layer + 1, one(seg), 1)
                    queries(following, layer + 1, (2, segments))

    layer, hidden = LAYERS - 1, hiddens[LAYERS - 1]
    w_copy(3, layer).wait()
    w_copy(4, layer).wait()
    late, late_piece = range(2, segments)[::-1], (2, segments)
    with scope("halo_late"):
        for seg in late:
            wait_halo(layer, seg)
    with scope("attend_late"):
        results = [scores(layer, seg) for seg in late]
        for seg, result in zip(late, results):
            weigh(layer, seg, soften(result))
    for seg in late:
        pair_copy(layer, seg).start()
    with scope("own_late"):
        own_half(hidden, layer, late_piece)
        queries(hidden, layer, (0, 2))
    with scope("halo_1"):
        wait_halo(layer, 1)
    with scope("pair_late"):
        for seg in late:
            pair_copy(layer, seg).wait_recv()
    with scope("block_1_late"):
        result = scores(layer, 1)
        other_half(layer, late_piece)
        weigh(layer, 1, soften(result))
        finish(layer, late_piece)
    pair_copy(layer, 1).start()
    with scope("k_0"):
        wait_halo(layer, 0, 0)
    with scope("soften_0_own_1"):
        result = scores(layer, 0)
        own_half(hidden, layer, one(1))
        softened = soften(result)
    with scope("v_0"):
        wait_halo(layer, 0, 1)
    with scope("weigh_0"):
        weigh(layer, 0, softened)
    pair_copy(layer, 0).start()
    with scope("pair_1"):
        pair_copy(layer, 1).wait_recv()
    with scope("finish_1"):
        other_half(layer, one(1))
        own_half(hidden, layer, one(0))
        finish(layer, one(1))
    with scope("pair_0"):
        pair_copy(layer, 0).wait_recv()
    with scope("finish_0"):
        other_half(layer, one(0))
        finish(layer, one(0))

    for layer in range(LAYERS):
        for seg in range(segments):
            pair_copy(layer, seg).wait_send()

    @pl.when(has_next)
    def _():
        for layer in range(LAYERS):
            for seg in range(segments):
                for kind in range(2):
                    halo_copy(kind, layer, seg).wait_send()


def body(
    sp_count, tokens, query_weight, key_weight, value_weight, out_weight, rel_table, norm_gain,
    norm_bias,
):
    rows, model = tokens.shape
    width = query_weight.shape[2]
    heads = rel_table.shape[1]
    reach = LEFT * SEG
    segments = rows // SEG
    wide = -(-(reach + 2 * SEG - 1) // LANES) * LANES
    size = -(-rel_table.shape[2] // LANES) * LANES
    hbm = pl.BlockSpec(memory_space=pltpu.MemorySpace.HBM)
    vmem = pl.BlockSpec(memory_space=pltpu.VMEM)
    bf16 = jnp.bfloat16
    return pl.pallas_call(
        functools.partial(kernel, sp_count, heads),
        out_shape=jax.ShapeDtypeStruct((rows, model // 2), bf16),
        in_specs=[hbm] * 8,
        out_specs=vmem,
        scratch_shapes=[
            pltpu.VMEM((rows, model), bf16),
            pltpu.VMEM((rows, model), bf16),
            pltpu.VMEM(query_weight.shape, bf16),
            pltpu.VMEM(key_weight.shape, bf16),
            pltpu.VMEM(value_weight.shape, bf16),
            pltpu.VMEM((LAYERS, 2, width, model), bf16),
            pltpu.VMEM(rel_table.shape, jnp.float32),
            pltpu.VMEM(norm_gain.shape, jnp.float32),
            pltpu.VMEM(norm_bias.shape, jnp.float32),
            pltpu.VMEM((LAYERS, rows, width), bf16),
            pltpu.VMEM((LAYERS, reach + rows, width), bf16),
            pltpu.VMEM((LAYERS, reach + rows, width), bf16),
            pltpu.VMEM((LAYERS, rows, width), bf16),
            pltpu.VMEM((LAYERS, rows, width), bf16),
            pltpu.VMEM((rows, model), jnp.float32),
            pltpu.VMEM((LAYERS, heads * SEG, wide), jnp.float32),
            pltpu.VMEM((-(-LAYERS * heads // 8) * 8, size), jnp.float32),
            pltpu.SemaphoreType.DMA((2,)),
            pltpu.SemaphoreType.DMA((2, CHUNKS)),
            pltpu.SemaphoreType.DMA((5, LAYERS)),
            pltpu.SemaphoreType.DMA((3,)),
            pltpu.SemaphoreType.DMA((2, LAYERS, segments)),
            pltpu.SemaphoreType.DMA((2, LAYERS, segments)),
            pltpu.SemaphoreType.DMA((LAYERS, segments)),
            pltpu.SemaphoreType.DMA((LAYERS, segments)),
        ],
        compiler_params=pltpu.CompilerParams(
            collective_id=0, has_side_effects=True, vmem_limit_bytes=56000000
        ),
    )(
        *(
            pltpu.with_memory_space_constraint(operand, pltpu.MemorySpace.HBM)
            for operand in (
                tokens,
                query_weight,
                key_weight,
                value_weight,
                out_weight,
                rel_table,
                norm_gain,
                norm_bias,
            )
        )
    )


def solution(mesh):
    return jax.shard_map(
        functools.partial(body, mesh.shape["sp"]),
        mesh=mesh,
        in_specs=(
            P("sp", None),
            P(None, None, "tp"),
            P(None, None, "tp"),
            P(None, None, "tp"),
            P(),
            P(None, "tp", None),
            P(),
            P(),
        ),
        out_specs=P("sp", "tp"),
        check_vma=False,
    )
```

```python
import functools

import jax
import jax.numpy as jnp
from jax import lax
from jax.experimental import pallas as pl
from jax.experimental.pallas import tpu as pltpu
from jax.sharding import PartitionSpec as P

SEG = 64
LEFT = 4
CLIP = 128
LAYERS = 2
LANES = 128
CHUNKS = 4

residual_scale = 2.0**0.5
norm_eps = 1e-05
masked_score = -1e30
MESH = pl.DeviceIdType.MESH


def kernel(
    sp_count,
    heads,
    tokens,
    wq_hbm,
    wk_hbm,
    wv_hbm,
    wo_hbm,
    table_hbm,
    gain_hbm,
    shift_hbm,
    out,
    x0,
    x1,
    wq,
    wk,
    wv,
    wo,
    table,
    gain,
    shift,
    query,
    kx,
    vx,
    att,
    peer,
    total,
    bias,
    padded,
    x_sem,
    first_sem,
    w_sem,
    small_sem,
    halo_send,
    halo_recv,
    pair_send,
    pair_recv,
):
    rows, model = x0.shape
    width = query.shape[2]
    head_size = width // heads
    reach = LEFT * SEG
    band = reach + SEG
    segments = rows // SEG
    sp = lax.axis_index("sp")
    tp = lax.axis_index("tp")
    has_next = sp < sp_count - 1
    has_prev = sp > 0

    def first_copy(kind, index):
        size = model // CHUNKS
        part = pl.ds(index * size, size)
        return pltpu.make_async_copy(
            (wk_hbm, wv_hbm)[kind].at[0, part],
            (wk, wv)[kind].at[0, part],
            first_sem.at[kind, index],
        )

    def w_copy(kind, layer):
        if kind < 3:
            source = (wk_hbm, wv_hbm, wq_hbm)[kind].at[layer]
            target = (wk, wv, wq)[kind].at[layer]
        else:
            owner = (tp, 1 - tp)[kind - 3]
            part = pl.ds(pl.multiple_of(owner * width, width), width)
            source = wo_hbm.at[layer, part]
            target = wo.at[layer, kind - 3]
        return pltpu.make_async_copy(source, target, w_sem.at[kind, layer])

    def x_copy(index, first, count):
        part = pl.ds(first, count)
        return pltpu.make_async_copy(tokens.at[part], x0.at[part], x_sem.at[index])

    x_last = x_copy(0, rows - SEG, SEG)
    x_rest = x_copy(1, 0, rows - SEG)
    small = [
        pltpu.make_async_copy(source, target, small_sem.at[index])
        for index, (source, target) in enumerate(
            ((table_hbm, table), (gain_hbm, gain), (shift_hbm, shift))
        )
    ]

    def halo_copy(kind, layer, seg):
        buffer = (kx, vx)[kind]
        return pltpu.make_async_remote_copy(
            src_ref=buffer.at[layer, pl.ds(reach + seg * SEG, SEG)],
            dst_ref=buffer.at[layer, pl.ds(seg * SEG, SEG)],
            send_sem=halo_send.at[kind, layer, seg],
            recv_sem=halo_recv.at[kind, layer, seg],
            device_id=(jnp.minimum(sp + 1, sp_count - 1), tp),
            device_id_type=MESH,
        )

    def pair_copy(layer, seg):
        part = pl.ds(seg * SEG, SEG)
        return pltpu.make_async_remote_copy(
            src_ref=att.at[layer, part],
            dst_ref=peer.at[layer, part],
            send_sem=pair_send.at[layer, seg],
            recv_sem=pair_recv.at[layer, seg],
            device_id=(sp, 1 - tp),
            device_id_type=MESH,
        )

    barrier = pltpu.get_barrier_semaphore()
    pl.semaphore_signal(barrier, inc=1, device_id=(sp, 1 - tp), device_id_type=MESH)

    @pl.when(has_prev)
    def _():
        pl.semaphore_signal(barrier, inc=1, device_id=(sp - 1, tp), device_id_type=MESH)

    x_last.start()
    first = [first_copy(kind, index) for kind in range(2) for index in range(CHUNKS)]
    for copy in first[:CHUNKS]:
        copy.start()
    pl.delay(120)
    for copy in first[CHUNKS:]:
        copy.start()
    x_rest.start()
    w_copy(2, 0).start()

    @pl.when(jnp.logical_not(has_prev))
    def _():
        for layer in range(LAYERS):
            kx[layer, :reach, :] = jnp.zeros((reach, width), jnp.bfloat16)
            vx[layer, :reach, :] = jnp.zeros((reach, width), jnp.bfloat16)

    def build_bias():
        wide = bias.shape[2]
        size = padded.shape[1]
        padded[...] = jnp.zeros_like(padded)
        for layer in range(LAYERS):
            padded[layer * heads : (layer + 1) * heads, : table.shape[2]] = table[layer]
        place = lax.broadcasted_iota(jnp.int32, (size, wide), 1)
        source = lax.broadcasted_iota(jnp.int32, (size, wide), 0)
        onehot = (jnp.clip(band - 1 - place, -CLIP, CLIP) + CLIP == source).astype(jnp.float32)
        by_offset = jnp.dot(
            padded[...],
            onehot,
            precision=lax.Precision.HIGHEST,
            preferred_element_type=jnp.float32,
        )
        for layer in range(LAYERS):
            for h in range(heads):
                line = by_offset[layer * heads + h : layer * heads + h + 1, :]
                skewed = pltpu.roll(
                    jnp.broadcast_to(line, (SEG, wide)), wide - SEG + 1, 1, stride=1, stride_axis=0
                )
                bias[layer, h * SEG : (h + 1) * SEG, :] = skewed

    def rows_of(piece):
        return slice(piece[0] * SEG, piece[1] * SEG)

    def project(hidden, layer, part, kind):
        weight = (wk, wv, wq)[kind]
        return jnp.dot(
            hidden[part, :], weight[layer], preferred_element_type=jnp.float32
        ).astype(jnp.bfloat16)

    def keys_values(hidden, layer, piece):
        part = rows_of(piece)
        target = slice(reach + part.start, reach + part.stop)
        kx[layer, target, :] = project(hidden, layer, part, 0)
        vx[layer, target, :] = project(hidden, layer, part, 1)

    def send(layer, piece, core):
        @pl.when(has_next & (tp == core))
        def _():
            for seg in range(*piece)[::-1]:
                halo_copy(0, layer, seg).start()
                halo_copy(1, layer, seg).start()

    def project_split(hidden, layer, part, kind):
        weight = (wk, wv, wq)[kind]
        return [
            jnp.dot(
                hidden[part, :],
                weight[layer, :, first : first + LANES],
                preferred_element_type=jnp.float32,
            ).astype(jnp.bfloat16)
            for first in range(0, width, LANES)
        ]

    def store_keys(hidden, layer, seg):
        target = slice(reach + seg * SEG, reach + (seg + 1) * SEG)
        for group, block in enumerate(
            project_split(hidden, layer, slice(seg * SEG, (seg + 1) * SEG), 0)
        ):
            kx[layer, target, group * LANES : (group + 1) * LANES] = block

    def values(hidden, layer, seg):
        target = slice(reach + seg * SEG, reach + (seg + 1) * SEG)
        for group, block in enumerate(
            project_split(hidden, layer, slice(seg * SEG, (seg + 1) * SEG), 1)
        ):
            vx[layer, target, group * LANES : (group + 1) * LANES] = block

        @pl.when(has_next)
        def _():
            halo_copy(1, layer, seg).start()

    def queries_split(hidden, layer, seg):
        part = slice(seg * SEG, (seg + 1) * SEG)
        for group, block in enumerate(project_split(hidden, layer, part, 2)):
            query[layer, part, group * LANES : (group + 1) * LANES] = block * jnp.bfloat16(
                head_size**-0.5
            )

    def queries(hidden, layer, piece):
        first, last = piece[0] * SEG, piece[1] * SEG
        middle = (first + last) // 2 if last - first > SEG else last
        for part in (slice(first, middle), slice(middle, last)):
            if part.start == part.stop:
                continue
            query[layer, part, :] = project(hidden, layer, part, 2) * jnp.bfloat16(
                head_size**-0.5
            )

    def wait_halo(layer, seg, kind=None):
        @pl.when(has_prev)
        def _():
            for each in (0, 1) if kind is None else (kind,):
                halo_copy(each, layer, seg).wait_recv()

    pair = LANES // head_size
    lane = lax.broadcasted_iota(jnp.int32, (1, LANES), 1)
    in_pair = [
        (lane >= h * head_size) & (lane < (h + 1) * head_size) for h in range(pair)
    ]

    def scores(layer, seg):
        column = lax.broadcasted_iota(jnp.int32, (1, band), 1)
        outside = (column < reach - seg * SEG) & jnp.logical_not(has_prev)
        results = []
        for group in range(width // LANES):
            lanes = slice(group * LANES, (group + 1) * LANES)
            block = query[layer, seg * SEG : (seg + 1) * SEG, lanes]
            stacked = jnp.concatenate(
                [jnp.where(in_pair[h], block, jnp.zeros_like(block)) for h in range(pair)], axis=0
            )
            raw = lax.dot_general(
                stacked,
                kx[layer, seg * SEG : seg * SEG + band, lanes],
                (((1,), (1,)), ((), ())),
                preferred_element_type=jnp.float32,
            )
            lines = slice(group * pair * SEG, (group + 1) * pair * SEG)
            results.append(jnp.where(outside, masked_score, raw + bias[layer, lines, :band]))
        return results

    def soften(results):
        softened = []
        for raw in results:
            expo = jnp.exp(raw - jnp.max(raw, -1, keepdims=True))
            norm = jnp.sum(expo, -1, keepdims=True)
            softened.append((expo.astype(jnp.bfloat16), 1.0 / norm))
        return softened

    def weigh(layer, seg, softened):
        for group, (expo, inverse) in enumerate(softened):
            lanes = slice(group * LANES, (group + 1) * LANES)
            mixed = jnp.dot(
                expo,
                vx[layer, seg * SEG : seg * SEG + band, lanes],
                preferred_element_type=jnp.float32,
            )
            mixed = mixed * inverse
            own = mixed[:SEG, :]
            for h in range(1, pair):
                own = jnp.where(in_pair[h], mixed[h * SEG : (h + 1) * SEG, :], own)
            att[layer, seg * SEG : (seg + 1) * SEG, lanes] = own.astype(jnp.bfloat16)

    def half(layer, piece, source, index):
        return jnp.dot(
            source[layer, rows_of(piece), :],
            wo[layer, index],
            preferred_element_type=jnp.float32,
        )

    def own_half(hidden, layer, piece):
        part = rows_of(piece)
        total[part, :] = half(layer, piece, att, 0) + residual_scale * hidden[part, :].astype(
            jnp.float32
        )

    def other_half(layer, piece):
        total[rows_of(piece), :] += half(layer, piece, peer, 1)

    def finish(layer, piece):
        step = 8
        part = rows_of(piece)
        for r in range(part.start, part.stop, step):
            here = slice(r, r + step)
            value = total[here, :]
            mean = jnp.sum(value, -1, keepdims=True) * (1.0 / model)
            centred = value - mean
            variance = jnp.sum(centred * centred, -1, keepdims=True) * (1.0 / model)
            scale = lax.rsqrt(variance + norm_eps)
            if layer < LAYERS - 1:
                x1[here, :] = (
                    centred * scale * gain[layer : layer + 1, :] + shift[layer : layer + 1, :]
                ).astype(jnp.bfloat16)
            else:
                cols = pl.ds(pl.multiple_of(tp * (model // 2), model // 2), model // 2)
                out[here, :] = (
                    (total[here, cols] - mean) * scale * gain[layer : layer + 1, cols]
                    + shift[layer : layer + 1, cols]
                ).astype(jnp.bfloat16)

    last = segments - 1
    scope = jax.named_scope
    with scope("x_last"):
        x_last.wait()
    with scope("w_k"):
        for copy in first[:CHUNKS]:
            copy.wait()
    with scope("k_last"):
        store_keys(x0, 0, last)
    with scope("barrier"):
        pl.semaphore_wait(barrier, 1 + has_next.astype(jnp.int32))

    @pl.when(has_next)
    def _():
        halo_copy(0, 0, last).start()

    with scope("w_v"):
        for copy in first[CHUNKS:]:
            copy.wait()
    with scope("v_last"):
        values(x0, 0, last)
    with scope("x_rest"):
        x_rest.wait()
    for copy in (*small, w_copy(3, 0), w_copy(4, 0)):
        copy.start()
    with scope("kv_next"):
        keys_values(x0, 0, (last - 1, last))
        send(0, (last - 1, last), 0)
    with scope("kv_rest"):
        keys_values(x0, 0, (0, last - 1))
        send(0, (0, last - 1), 0)
    w_copy(2, 0).wait()
    for kind in range(2):
        w_copy(kind, 1).start()
    with scope("queries"):
        queries(x0, 0, (0, segments))
    send(0, (0, last), 1)
    for copy in small:
        copy.wait()
    with scope("bias"):
        build_bias()
    for kind in range(2, 5):
        w_copy(kind, 1).start()
    w_copy(3, 0).wait()
    w_copy(4, 0).wait()

    def one(seg):
        return (seg, seg + 1)

    hiddens = (x0, x1)
    for layer in range(LAYERS - 1):
        hidden, following = hiddens[layer], hiddens[layer + 1]
        with scope(f"k_{layer}_{last}"):
            wait_halo(layer, last, 0)
        with scope(f"soften_{layer}_{last}"):
            softened = soften(scores(layer, last))
        with scope(f"v_{layer}_{last}"):
            wait_halo(layer, last, 1)
        with scope(f"weigh_{layer}_{last}"):
            weigh(layer, last, softened)
        pair_copy(layer, last).start()
        with scope(f"own_{layer}_{last}"):
            own_half(hidden, layer, one(last))
        for seg in range(segments)[::-1]:
            if seg > 0:
                with scope(f"halo_{layer}_{seg - 1}"):
                    wait_halo(layer, seg - 1)
            with scope(f"pair_{layer}_{seg}"):
                pair_copy(layer, seg).wait_recv()
            if seg == last:
                with scope(f"w_{layer}"):
                    for kind in range(3):
                        w_copy(kind, layer + 1).wait()
            with scope(f"block_{layer}_{seg}"):
                if seg > 0:
                    results = scores(layer, seg - 1)
                other_half(layer, one(seg))
                if seg > 0:
                    weigh(layer, seg - 1, soften(results))
            if seg > 0:
                pair_copy(layer, seg - 1).start()
            with scope(f"kv_{layer}_{seg}"):
                if seg > 0:
                    own_half(hidden, layer, one(seg - 1))
                finish(layer, one(seg))
                keys_values(following, layer + 1, one(seg))
                send(layer + 1, one(seg), 0)
                if seg > 0:
                    send(layer + 1, one(seg), 1)
            if seg == 0:
                with scope(f"q_{layer}_{seg}"):
                    send(layer + 1, one(seg), 1)
                    queries(following, layer + 1, (2, segments))

    layer, hidden = LAYERS - 1, hiddens[LAYERS - 1]
    w_copy(3, layer).wait()
    w_copy(4, layer).wait()
    late, late_piece = range(2, segments)[::-1], (2, segments)
    with scope("halo_late"):
        for seg in late:
            wait_halo(layer, seg)
    with scope("attend_late"):
        results = [scores(layer, seg) for seg in late]
        for seg, result in zip(late, results):
            weigh(layer, seg, soften(result))
    for seg in late:
        pair_copy(layer, seg).start()
    with scope("own_late"):
        own_half(hidden, layer, late_piece)
        queries(hidden, layer, (0, 2))
    with scope("halo_1"):
        wait_halo(layer, 1)
    with scope("pair_late"):
        for seg in late:
            pair_copy(layer, seg).wait_recv()
    with scope("block_1_late"):
        result = scores(layer, 1)
        other_half(layer, late_piece)
        weigh(layer, 1, soften(result))
        finish(layer, late_piece)
    pair_copy(layer, 1).start()
    with scope("k_0"):
        wait_halo(layer, 0, 0)
    with scope("soften_0_own_1"):
        result = scores(layer, 0)
        own_half(hidden, layer, one(1))
        softened = soften(result)
    with scope("v_0"):
        wait_halo(layer, 0, 1)
    with scope("weigh_0"):
        weigh(layer, 0, softened)
    pair_copy(layer, 0).start()
    with scope("pair_1"):
        pair_copy(layer, 1).wait_recv()
    with scope("finish_1"):
        other_half(layer, one(1))
        own_half(hidden, layer, one(0))
        finish(layer, one(1))
    with scope("pair_0"):
        pair_copy(layer, 0).wait_recv()
    with scope("finish_0"):
        other_half(layer, one(0))
        finish(layer, one(0))

    for layer in range(LAYERS):
        for seg in range(segments):
            pair_copy(layer, seg).wait_send()

    @pl.when(has_next)
    def _():
        for layer in range(LAYERS):
            for seg in range(segments):
                for kind in range(2):
                    halo_copy(kind, layer, seg).wait_send()


def body(
    sp_count, tokens, query_weight, key_weight, value_weight, out_weight, rel_table, norm_gain,
    norm_bias,
):
    rows, model = tokens.shape
    width = query_weight.shape[2]
    heads = rel_table.shape[1]
    reach = LEFT * SEG
    segments = rows // SEG
    wide = -(-(reach + 2 * SEG - 1) // LANES) * LANES
    size = -(-rel_table.shape[2] // LANES) * LANES
    hbm = pl.BlockSpec(memory_space=pltpu.MemorySpace.HBM)
    vmem = pl.BlockSpec(memory_space=pltpu.VMEM)
    bf16 = jnp.bfloat16
    return pl.pallas_call(
        functools.partial(kernel, sp_count, heads),
        out_shape=jax.ShapeDtypeStruct((rows, model // 2), bf16),
        in_specs=[hbm] * 8,
        out_specs=vmem,
        scratch_shapes=[
            pltpu.VMEM((rows, model), bf16),
            pltpu.VMEM((rows, model), bf16),
            pltpu.VMEM(query_weight.shape, bf16),
            pltpu.VMEM(key_weight.shape, bf16),
            pltpu.VMEM(value_weight.shape, bf16),
            pltpu.VMEM((LAYERS, 2, width, model), bf16),
            pltpu.VMEM(rel_table.shape, jnp.float32),
            pltpu.VMEM(norm_gain.shape, jnp.float32),
            pltpu.VMEM(norm_bias.shape, jnp.float32),
            pltpu.VMEM((LAYERS, rows, width), bf16),
            pltpu.VMEM((LAYERS, reach + rows, width), bf16),
            pltpu.VMEM((LAYERS, reach + rows, width), bf16),
            pltpu.VMEM((LAYERS, rows, width), bf16),
            pltpu.VMEM((LAYERS, rows, width), bf16),
            pltpu.VMEM((rows, model), jnp.float32),
            pltpu.VMEM((LAYERS, heads * SEG, wide), jnp.float32),
            pltpu.VMEM((-(-LAYERS * heads // 8) * 8, size), jnp.float32),
            pltpu.SemaphoreType.DMA((2,)),
            pltpu.SemaphoreType.DMA((2, CHUNKS)),
            pltpu.SemaphoreType.DMA((5, LAYERS)),
            pltpu.SemaphoreType.DMA((3,)),
            pltpu.SemaphoreType.DMA((2, LAYERS, segments)),
            pltpu.SemaphoreType.DMA((2, LAYERS, segments)),
            pltpu.SemaphoreType.DMA((LAYERS, segments)),
            pltpu.SemaphoreType.DMA((LAYERS, segments)),
        ],
        compiler_params=pltpu.CompilerParams(
            collective_id=0, has_side_effects=True, vmem_limit_bytes=56000000
        ),
    )(
        *(
            pltpu.with_memory_space_constraint(operand, pltpu.MemorySpace.HBM)
            for operand in (
                tokens,
                query_weight,
                key_weight,
                value_weight,
                out_weight,
                rel_table,
                norm_gain,
                norm_bias,
            )
        )
    )


def solution(mesh):
    return jax.shard_map(
        functools.partial(body, mesh.shape["sp"]),
        mesh=mesh,
        in_specs=(
            P("sp", None),
            P(None, None, "tp"),
            P(None, None, "tp"),
            P(None, None, "tp"),
            P(),
            P(None, "tp", None),
            P(),
            P(),
        ),
        out_specs=P("sp", "tp"),
        check_vma=False,
    )
```

```python
import functools

import jax
import jax.numpy as jnp
from jax import lax
from jax.experimental import pallas as pl
from jax.experimental.pallas import tpu as pltpu
from jax.sharding import PartitionSpec as P

SEG = 64
LEFT = 4
CLIP = 128
LAYERS = 2
LANES = 128
CHUNKS = 4

residual_scale = 2.0**0.5
norm_eps = 1e-05
masked_score = -1e30
MESH = pl.DeviceIdType.MESH


def kernel(
    sp_count,
    heads,
    tokens,
    wq_hbm,
    wk_hbm,
    wv_hbm,
    wo_hbm,
    table_hbm,
    gain_hbm,
    shift_hbm,
    out,
    x0,
    x1,
    wq,
    wk,
    wv,
    wo,
    table,
    gain,
    shift,
    query,
    kx,
    vx,
    att,
    peer,
    total,
    bias,
    padded,
    x_sem,
    first_sem,
    w_sem,
    small_sem,
    halo_send,
    halo_recv,
    pair_send,
    pair_recv,
):
    rows, model = x0.shape
    width = query.shape[2]
    head_size = width // heads
    reach = LEFT * SEG
    band = reach + SEG
    segments = rows // SEG
    sp = lax.axis_index("sp")
    tp = lax.axis_index("tp")
    has_next = sp < sp_count - 1
    has_prev = sp > 0

    def first_copy(kind, index):
        size = model // CHUNKS
        part = pl.ds(index * size, size)
        return pltpu.make_async_copy(
            (wk_hbm, wv_hbm)[kind].at[0, part],
            (wk, wv)[kind].at[0, part],
            first_sem.at[kind, index],
        )

    def w_copy(kind, layer):
        if kind < 3:
            source = (wk_hbm, wv_hbm, wq_hbm)[kind].at[layer]
            target = (wk, wv, wq)[kind].at[layer]
        else:
            owner = (tp, 1 - tp)[kind - 3]
            part = pl.ds(pl.multiple_of(owner * width, width), width)
            source = wo_hbm.at[layer, part]
            target = wo.at[layer, kind - 3]
        return pltpu.make_async_copy(source, target, w_sem.at[kind, layer])

    def x_copy(index, first, count):
        part = pl.ds(first, count)
        return pltpu.make_async_copy(tokens.at[part], x0.at[part], x_sem.at[index])

    x_last = x_copy(0, rows - SEG, SEG)
    x_rest = x_copy(1, 0, rows - SEG)
    small = [
        pltpu.make_async_copy(source, target, small_sem.at[index])
        for index, (source, target) in enumerate(
            ((table_hbm, table), (gain_hbm, gain), (shift_hbm, shift))
        )
    ]

    def halo_copy(kind, layer, seg):
        buffer = (kx, vx)[kind]
        return pltpu.make_async_remote_copy(
            src_ref=buffer.at[layer, pl.ds(reach + seg * SEG, SEG)],
            dst_ref=buffer.at[layer, pl.ds(seg * SEG, SEG)],
            send_sem=halo_send.at[kind, layer, seg],
            recv_sem=halo_recv.at[kind, layer, seg],
            device_id=(jnp.minimum(sp + 1, sp_count - 1), tp),
            device_id_type=MESH,
        )

    def pair_copy(layer, seg):
        part = pl.ds(seg * SEG, SEG)
        return pltpu.make_async_remote_copy(
            src_ref=att.at[layer, part],
            dst_ref=peer.at[layer, part],
            send_sem=pair_send.at[layer, seg],
            recv_sem=pair_recv.at[layer, seg],
            device_id=(sp, 1 - tp),
            device_id_type=MESH,
        )

    barrier = pltpu.get_barrier_semaphore()
    pl.semaphore_signal(barrier, inc=1, device_id=(sp, 1 - tp), device_id_type=MESH)

    @pl.when(has_prev)
    def _():
        pl.semaphore_signal(barrier, inc=1, device_id=(sp - 1, tp), device_id_type=MESH)

    x_last.start()
    first = [first_copy(kind, index) for kind in range(2) for index in range(CHUNKS)]
    for copy in first[:CHUNKS]:
        copy.start()
    pl.delay(120)
    for copy in first[CHUNKS:]:
        copy.start()
    x_rest.start()
    w_copy(2, 0).start()

    @pl.when(jnp.logical_not(has_prev))
    def _():
        for layer in range(LAYERS):
            kx[layer, :reach, :] = jnp.zeros((reach, width), jnp.bfloat16)
            vx[layer, :reach, :] = jnp.zeros((reach, width), jnp.bfloat16)

    def build_bias():
        wide = bias.shape[2]
        size = padded.shape[1]
        padded[...] = jnp.zeros_like(padded)
        for layer in range(LAYERS):
            padded[layer * heads : (layer + 1) * heads, : table.shape[2]] = table[layer]
        place = lax.broadcasted_iota(jnp.int32, (size, wide), 1)
        source = lax.broadcasted_iota(jnp.int32, (size, wide), 0)
        onehot = (jnp.clip(band - 1 - place, -CLIP, CLIP) + CLIP == source).astype(jnp.float32)
        by_offset = jnp.dot(
            padded[...],
            onehot,
            precision=lax.Precision.HIGHEST,
            preferred_element_type=jnp.float32,
        )
        for layer in range(LAYERS):
            for h in range(heads):
                line = by_offset[layer * heads + h : layer * heads + h + 1, :]
                skewed = pltpu.roll(
                    jnp.broadcast_to(line, (SEG, wide)), wide - SEG + 1, 1, stride=1, stride_axis=0
                )
                bias[layer, h * SEG : (h + 1) * SEG, :] = skewed

    def rows_of(piece):
        return slice(piece[0] * SEG, piece[1] * SEG)

    def project(hidden, layer, part, kind):
        weight = (wk, wv, wq)[kind]
        return jnp.dot(
            hidden[part, :], weight[layer], preferred_element_type=jnp.float32
        ).astype(jnp.bfloat16)

    def keys_values(hidden, layer, piece):
        part = rows_of(piece)
        target = slice(reach + part.start, reach + part.stop)
        kx[layer, target, :] = project(hidden, layer, part, 0)
        vx[layer, target, :] = project(hidden, layer, part, 1)

    def send(layer, piece, core):
        @pl.when(has_next & (tp == core))
        def _():
            for seg in range(*piece)[::-1]:
                halo_copy(0, layer, seg).start()
                halo_copy(1, layer, seg).start()

    def project_split(hidden, layer, part, kind):
        weight = (wk, wv, wq)[kind]
        return [
            jnp.dot(
                hidden[part, :],
                weight[layer, :, first : first + LANES],
                preferred_element_type=jnp.float32,
            ).astype(jnp.bfloat16)
            for first in range(0, width, LANES)
        ]

    def store_keys(hidden, layer, seg):
        target = slice(reach + seg * SEG, reach + (seg + 1) * SEG)
        for group, block in enumerate(
            project_split(hidden, layer, slice(seg * SEG, (seg + 1) * SEG), 0)
        ):
            kx[layer, target, group * LANES : (group + 1) * LANES] = block

    def values(hidden, layer, seg):
        target = slice(reach + seg * SEG, reach + (seg + 1) * SEG)
        for group, block in enumerate(
            project_split(hidden, layer, slice(seg * SEG, (seg + 1) * SEG), 1)
        ):
            vx[layer, target, group * LANES : (group + 1) * LANES] = block

        @pl.when(has_next)
        def _():
            halo_copy(1, layer, seg).start()

    def queries_split(hidden, layer, seg):
        part = slice(seg * SEG, (seg + 1) * SEG)
        for group, block in enumerate(project_split(hidden, layer, part, 2)):
            query[layer, part, group * LANES : (group + 1) * LANES] = block * jnp.bfloat16(
                head_size**-0.5
            )

    def queries(hidden, layer, piece):
        first, last = piece[0] * SEG, piece[1] * SEG
        middle = (first + last) // 2 if last - first > SEG else last
        for part in (slice(first, middle), slice(middle, last)):
            if part.start == part.stop:
                continue
            query[layer, part, :] = project(hidden, layer, part, 2) * jnp.bfloat16(
                head_size**-0.5
            )

    def wait_halo(layer, seg, kind=None):
        @pl.when(has_prev)
        def _():
            for each in (0, 1) if kind is None else (kind,):
                halo_copy(each, layer, seg).wait_recv()

    pair = LANES // head_size
    lane = lax.broadcasted_iota(jnp.int32, (1, LANES), 1)
    in_pair = [
        (lane >= h * head_size) & (lane < (h + 1) * head_size) for h in range(pair)
    ]

    def scores(layer, seg):
        column = lax.broadcasted_iota(jnp.int32, (1, band), 1)
        outside = (column < reach - seg * SEG) & jnp.logical_not(has_prev)
        results = []
        for group in range(width // LANES):
            lanes = slice(group * LANES, (group + 1) * LANES)
            block = query[layer, seg * SEG : (seg + 1) * SEG, lanes]
            stacked = jnp.concatenate(
                [jnp.where(in_pair[h], block, jnp.zeros_like(block)) for h in range(pair)], axis=0
            )
            raw = lax.dot_general(
                stacked,
                kx[layer, seg * SEG : seg * SEG + band, lanes],
                (((1,), (1,)), ((), ())),
                preferred_element_type=jnp.float32,
            )
            lines = slice(group * pair * SEG, (group + 1) * pair * SEG)
            results.append(jnp.where(outside, masked_score, raw + bias[layer, lines, :band]))
        return results

    def soften(results):
        softened = []
        for raw in results:
            expo = jnp.exp(raw - jnp.max(raw, -1, keepdims=True))
            norm = jnp.sum(expo, -1, keepdims=True)
            softened.append((expo.astype(jnp.bfloat16), 1.0 / norm))
        return softened

    def weigh(layer, seg, softened):
        for group, (expo, inverse) in enumerate(softened):
            lanes = slice(group * LANES, (group + 1) * LANES)
            mixed = jnp.dot(
                expo,
                vx[layer, seg * SEG : seg * SEG + band, lanes],
                preferred_element_type=jnp.float32,
            )
            mixed = mixed * inverse
            own = mixed[:SEG, :]
            for h in range(1, pair):
                own = jnp.where(in_pair[h], mixed[h * SEG : (h + 1) * SEG, :], own)
            att[layer, seg * SEG : (seg + 1) * SEG, lanes] = own.astype(jnp.bfloat16)

    def half(layer, piece, source, index):
        return jnp.dot(
            source[layer, rows_of(piece), :],
            wo[layer, index],
            preferred_element_type=jnp.float32,
        )

    def own_half(hidden, layer, piece):
        part = rows_of(piece)
        total[part, :] = half(layer, piece, att, 0) + residual_scale * hidden[part, :].astype(
            jnp.float32
        )

    def other_half(layer, piece):
        total[rows_of(piece), :] += half(layer, piece, peer, 1)

    def finish(layer, piece):
        step = 8
        part = rows_of(piece)
        for r in range(part.start, part.stop, step):
            here = slice(r, r + step)
            value = total[here, :]
            mean = jnp.sum(value, -1, keepdims=True) * (1.0 / model)
            centred = value - mean
            variance = jnp.sum(centred * centred, -1, keepdims=True) * (1.0 / model)
            scale = lax.rsqrt(variance + norm_eps)
            if layer < LAYERS - 1:
                x1[here, :] = (
                    centred * scale * gain[layer : layer + 1, :] + shift[layer : layer + 1, :]
                ).astype(jnp.bfloat16)
            else:
                cols = pl.ds(pl.multiple_of(tp * (model // 2), model // 2), model // 2)
                out[here, :] = (
                    (total[here, cols] - mean) * scale * gain[layer : layer + 1, cols]
                    + shift[layer : layer + 1, cols]
                ).astype(jnp.bfloat16)

    last = segments - 1
    scope = jax.named_scope
    with scope("x_last"):
        x_last.wait()
    with scope("w_k"):
        for copy in first[:CHUNKS]:
            copy.wait()
    with scope("k_last"):
        store_keys(x0, 0, last)
    with scope("barrier"):
        pl.semaphore_wait(barrier, 1 + has_next.astype(jnp.int32))

    @pl.when(has_next)
    def _():
        halo_copy(0, 0, last).start()

    with scope("w_v"):
        for copy in first[CHUNKS:]:
            copy.wait()
    with scope("v_last"):
        values(x0, 0, last)
    with scope("x_rest"):
        x_rest.wait()
    for copy in (*small, w_copy(3, 0), w_copy(4, 0)):
        copy.start()
    with scope("kv_next"):
        keys_values(x0, 0, (last - 1, last))
        send(0, (last - 1, last), 0)
    with scope("kv_rest"):
        keys_values(x0, 0, (0, last - 1))
        send(0, (0, last - 1), 0)
    w_copy(2, 0).wait()
    for kind in range(2):
        w_copy(kind, 1).start()
    with scope("queries"):
        queries(x0, 0, (0, segments))
    send(0, (last - 1, last), 1)
    for copy in small:
        copy.wait()
    with scope("bias"):
        build_bias()
    send(0, (0, last - 1), 1)
    for kind in range(2, 5):
        w_copy(kind, 1).start()
    w_copy(3, 0).wait()
    w_copy(4, 0).wait()

    def one(seg):
        return (seg, seg + 1)

    hiddens = (x0, x1)
    for layer in range(LAYERS - 1):
        hidden, following = hiddens[layer], hiddens[layer + 1]
        with scope(f"k_{layer}_{last}"):
            wait_halo(layer, last, 0)
        with scope(f"soften_{layer}_{last}"):
            softened = soften(scores(layer, last))
        with scope(f"v_{layer}_{last}"):
            wait_halo(layer, last, 1)
        with scope(f"weigh_{layer}_{last}"):
            weigh(layer, last, softened)
        pair_copy(layer, last).start()
        with scope(f"own_{layer}_{last}"):
            own_half(hidden, layer, one(last))
        for seg in range(segments)[::-1]:
            if seg > 0:
                with scope(f"halo_{layer}_{seg - 1}"):
                    wait_halo(layer, seg - 1)
            with scope(f"pair_{layer}_{seg}"):
                pair_copy(layer, seg).wait_recv()
            if seg == last:
                with scope(f"w_{layer}"):
                    for kind in range(3):
                        w_copy(kind, layer + 1).wait()
            with scope(f"block_{layer}_{seg}"):
                if seg > 0:
                    results = scores(layer, seg - 1)
                other_half(layer, one(seg))
                if seg > 0:
                    weigh(layer, seg - 1, soften(results))
            if seg > 0:
                pair_copy(layer, seg - 1).start()
            with scope(f"kv_{layer}_{seg}"):
                if seg > 0:
                    own_half(hidden, layer, one(seg - 1))
                finish(layer, one(seg))
                keys_values(following, layer + 1, one(seg))
                send(layer + 1, one(seg), 0)
                if seg > 0:
                    send(layer + 1, one(seg), 1)
            if seg == 0:
                with scope(f"q_{layer}_{seg}"):
                    send(layer + 1, one(seg), 1)
                    queries(following, layer + 1, (2, segments))

    layer, hidden = LAYERS - 1, hiddens[LAYERS - 1]
    w_copy(3, layer).wait()
    w_copy(4, layer).wait()
    late, late_piece = range(2, segments)[::-1], (2, segments)
    with scope("halo_late"):
        for seg in late:
            wait_halo(layer, seg)
    with scope("attend_late"):
        results = [scores(layer, seg) for seg in late]
        for seg, result in zip(late, results):
            weigh(layer, seg, soften(result))
    for seg in late:
        pair_copy(layer, seg).start()
    with scope("own_late"):
        own_half(hidden, layer, late_piece)
        queries(hidden, layer, (0, 2))
    with scope("halo_1"):
        wait_halo(layer, 1)
    with scope("pair_late"):
        for seg in late:
            pair_copy(layer, seg).wait_recv()
    with scope("block_1_late"):
        result = scores(layer, 1)
        other_half(layer, late_piece)
        weigh(layer, 1, soften(result))
        finish(layer, late_piece)
    pair_copy(layer, 1).start()
    with scope("k_0"):
        wait_halo(layer, 0, 0)
    with scope("soften_0_own_1"):
        result = scores(layer, 0)
        own_half(hidden, layer, one(1))
        softened = soften(result)
    with scope("v_0"):
        wait_halo(layer, 0, 1)
    with scope("weigh_0"):
        weigh(layer, 0, softened)
    pair_copy(layer, 0).start()
    with scope("pair_1"):
        pair_copy(layer, 1).wait_recv()
    with scope("finish_1"):
        other_half(layer, one(1))
        own_half(hidden, layer, one(0))
        finish(layer, one(1))
    with scope("pair_0"):
        pair_copy(layer, 0).wait_recv()
    with scope("finish_0"):
        other_half(layer, one(0))
        finish(layer, one(0))

    for layer in range(LAYERS):
        for seg in range(segments):
            pair_copy(layer, seg).wait_send()

    @pl.when(has_next)
    def _():
        for layer in range(LAYERS):
            for seg in range(segments):
                for kind in range(2):
                    halo_copy(kind, layer, seg).wait_send()


def body(
    sp_count, tokens, query_weight, key_weight, value_weight, out_weight, rel_table, norm_gain,
    norm_bias,
):
    rows, model = tokens.shape
    width = query_weight.shape[2]
    heads = rel_table.shape[1]
    reach = LEFT * SEG
    segments = rows // SEG
    wide = -(-(reach + 2 * SEG - 1) // LANES) * LANES
    size = -(-rel_table.shape[2] // LANES) * LANES
    hbm = pl.BlockSpec(memory_space=pltpu.MemorySpace.HBM)
    vmem = pl.BlockSpec(memory_space=pltpu.VMEM)
    bf16 = jnp.bfloat16
    return pl.pallas_call(
        functools.partial(kernel, sp_count, heads),
        out_shape=jax.ShapeDtypeStruct((rows, model // 2), bf16),
        in_specs=[hbm] * 8,
        out_specs=vmem,
        scratch_shapes=[
            pltpu.VMEM((rows, model), bf16),
            pltpu.VMEM((rows, model), bf16),
            pltpu.VMEM(query_weight.shape, bf16),
            pltpu.VMEM(key_weight.shape, bf16),
            pltpu.VMEM(value_weight.shape, bf16),
            pltpu.VMEM((LAYERS, 2, width, model), bf16),
            pltpu.VMEM(rel_table.shape, jnp.float32),
            pltpu.VMEM(norm_gain.shape, jnp.float32),
            pltpu.VMEM(norm_bias.shape, jnp.float32),
            pltpu.VMEM((LAYERS, rows, width), bf16),
            pltpu.VMEM((LAYERS, reach + rows, width), bf16),
            pltpu.VMEM((LAYERS, reach + rows, width), bf16),
            pltpu.VMEM((LAYERS, rows, width), bf16),
            pltpu.VMEM((LAYERS, rows, width), bf16),
            pltpu.VMEM((rows, model), jnp.float32),
            pltpu.VMEM((LAYERS, heads * SEG, wide), jnp.float32),
            pltpu.VMEM((-(-LAYERS * heads // 8) * 8, size), jnp.float32),
            pltpu.SemaphoreType.DMA((2,)),
            pltpu.SemaphoreType.DMA((2, CHUNKS)),
            pltpu.SemaphoreType.DMA((5, LAYERS)),
            pltpu.SemaphoreType.DMA((3,)),
            pltpu.SemaphoreType.DMA((2, LAYERS, segments)),
            pltpu.SemaphoreType.DMA((2, LAYERS, segments)),
            pltpu.SemaphoreType.DMA((LAYERS, segments)),
            pltpu.SemaphoreType.DMA((LAYERS, segments)),
        ],
        compiler_params=pltpu.CompilerParams(
            collective_id=0, has_side_effects=True, vmem_limit_bytes=56000000
        ),
    )(
        *(
            pltpu.with_memory_space_constraint(operand, pltpu.MemorySpace.HBM)
            for operand in (
                tokens,
                query_weight,
                key_weight,
                value_weight,
                out_weight,
                rel_table,
                norm_gain,
                norm_bias,
            )
        )
    )


def solution(mesh):
    return jax.shard_map(
        functools.partial(body, mesh.shape["sp"]),
        mesh=mesh,
        in_specs=(
            P("sp", None),
            P(None, None, "tp"),
            P(None, None, "tp"),
            P(None, None, "tp"),
            P(),
            P(None, "tp", None),
            P(),
            P(),
        ),
        out_specs=P("sp", "tp"),
        check_vma=False,
    )
```
